32 devices in a mesh: sp: 8 (over z, x), tp: 4 (over y, core).
Axes of the slice: x: 2, y: 2, z: 4, core: 2. Of those that a mesh axis runs over, the one named last changes fastest.
Arguments:
- latent: bfloat16 [4096, 2048], P(('sp', 'tp')), may hold values from -6 to 6
- context: bfloat16 [512, 2048], P('sp'), may hold values from -6 to 6
- conditioning: float32 [2048], P('sp'), may hold values from -6 to 6
- context_conditioning: float32 [2048], P('sp'), may hold values from -6 to 6
- shift_weight: bfloat16 [2048, 2048], P('sp', 'tp'), may hold values from -0.25 to 0.25
- scale_weight: bfloat16 [2048, 2048], P('sp', 'tp'), may hold values from -0.25 to 0.25
- gate_weight: bfloat16 [2048, 2048], P('sp', 'tp'), may hold values from -0.25 to 0.25
- norm_gain: float32 [2048], replicated, may hold values from 0.1 to 1.9
- query_weight: bfloat16 [2048, 2048], P(None, 'tp'), may hold values from -0.125 to 0.125
- key_weight: bfloat16 [2048, 1024], P(None, 'tp'), may hold values from -0.125 to 0.125
- value_weight: bfloat16 [2048, 1024], P(None, 'tp'), may hold values from -0.125 to 0.125
- query_gain: float32 [64], replicated, may hold values from 2 to 64, as said below
- key_gain: float32 [64], replicated, may hold values from 0.1 to 1.9
- context_lift: float32 [32], P('tp'), may hold values from 1.5 to 3
- output_weight: bfloat16 [2048, 2048], P('tp'), may hold values from -0.125 to 0.125
Outputs:
- mixed: bfloat16 [4096, 2048], P(('sp', 'tp'))
The draws below stay inside these ranges and needn't reach their ends.
Inputs may be any that keep to these rules, and one draw needn't show every extreme that they name: `query_gain`: one gain for each channel of a head.
All inputs are finite; a program needn't handle non-finite values.
Results may differ from the reference program's by a relative error of at most 0.018.
The reference program's roundings to bfloat16 on the way count: a program that leaves them out, or rounds other values in their place, can miss the bound.
Values may be sent and summed in bfloat16 or wider, within the bound.
No kernel may reach another device: no remote copies, remote signals or barrier semaphores. Data moves between devices by JAX's collectives and lax.ppermute only.
A program may use at most 128 MiB of HBM per device.

```python
import math
import jax
import jax.numpy as jnp
from jax import lax

D = 2048
HEAD = 64
Q_HEADS = 32
KV_HEADS = 16
GRID = 64
CTX = 512
TOKENS = 4096


def draw_query_gain(key, part):
    base_key = jax.random.fold_in(key, 0)
    gains = jax.random.uniform(base_key, (HEAD,), jnp.float32, 2.0, 3.5)
    return gains


def block_scale(own_key, shape, cuts, smallest, largest):
    level = 1.0
    for dim, shards_of in cuts:
        steps = jax.random.uniform(jax.random.fold_in(jax.random.fold_in(own_key, 6), dim), (shards_of,), jnp.float32, smallest / len(cuts), largest / len(cuts))
        level = level * jnp.repeat(jnp.exp(steps), shape[dim] // shards_of).reshape((-1,) + (1,) * (len(shape) - 1 - dim))
    return level


def gaussian(key, shape, spread, reach, cuts=(), held_as=jnp.bfloat16):
    values = jax.random.normal(key, shape, jnp.float32) * spread
    if len(cuts) > 0:
        values = block_scale(key, shape, cuts, -0.22, 0.18) * values
    return jnp.clip(values, min=-reach, max=reach).astype(held_as)


def setup_inputs(seed: int = 0) -> dict:
    arg_keys = jax.random.split(jax.random.key(seed), 16)
    return {
        "latent": gaussian(arg_keys[0], (TOKENS, D), 1.0, 6.0, ((0, 32),)),
        "context": gaussian(arg_keys[1], (CTX, D), 1.0, 6.0, ((0, 8),)),
        "conditioning": gaussian(arg_keys[2], (D,), 1.0, 6.0, ((0, 8),), jnp.float32),
        "context_conditioning": gaussian(arg_keys[3], (D,), 1.0, 6.0, ((0, 8),), jnp.float32),
        "shift_weight": gaussian(arg_keys[4], (D, D), (D // 4) ** -0.5, 0.25, ((0, 8), (1, 4))),
        "scale_weight": gaussian(arg_keys[5], (D, D), (D // 4) ** -0.5, 0.25, ((0, 8), (1, 4))),
        "gate_weight": gaussian(arg_keys[6], (D, D), (D // 4) ** -0.5, 0.25, ((0, 8), (1, 4))),
        "norm_gain": jnp.clip(1.0 + 0.18 * jax.random.normal(arg_keys[7], (D,), jnp.float32), 0.1, 1.9),
        "query_weight": gaussian(arg_keys[8], (D, Q_HEADS * HEAD), D ** -0.5, 0.125, ((1, 4),)),
        "key_weight": gaussian(arg_keys[9], (D, KV_HEADS * HEAD), D ** -0.5, 0.125, ((1, 4),)),
        "value_weight": gaussian(arg_keys[10], (D, KV_HEADS * HEAD), D ** -0.5, 0.125, ((1, 4),)),
        "query_gain": draw_query_gain(jax.random.fold_in(arg_keys[15], 71), 0),
        "key_gain": jnp.clip(1.0 + 0.18 * jax.random.normal(arg_keys[12], (HEAD,), jnp.float32), 0.1, 1.9),
        "context_lift": jnp.clip(1.5 + 1.5 * jax.random.uniform(arg_keys[13], (Q_HEADS,), jnp.float32) ** block_scale(arg_keys[13], (Q_HEADS,), ((0, 4),), -0.2, 0.2), 1.5, 3.0),
        "output_weight": gaussian(arg_keys[14], (Q_HEADS * HEAD, D), (Q_HEADS * HEAD) ** -0.5, 0.125, ((0, 4),)),
    }


EPSILON = 1e-06
ROTARY_BASE = 10000.0

def normalize(values, gain):
    return values * lax.rsqrt(lax.optimization_barrier(jnp.mean(values * values, axis=-1, keepdims=True)) + EPSILON) * gain

def rotary_tables(offset, count):
    position = offset + jnp.arange(count, dtype=jnp.int32)
    grid_row = (position // GRID).astype(jnp.float32)
    grid_column = (position % GRID).astype(jnp.float32)
    quarter = HEAD // 4
    frequency = ROTARY_BASE ** (-jnp.arange(quarter, dtype=jnp.float32) / quarter)
    angles = jnp.concatenate([grid_row[:, None] * frequency, grid_column[:, None] * frequency], axis=1)
    return (jnp.repeat(jnp.cos(angles), 2, axis=1), jnp.repeat(jnp.sin(angles), 2, axis=1))

def rotate(values, cos_table, sin_table):
    pairs = values.reshape(values.shape[:-1] + (HEAD // 2, 2))
    turned = jnp.stack([-pairs[..., 1], pairs[..., 0]], axis=-1).reshape(values.shape)
    return values * cos_table[:, None, :] + turned * sin_table[:, None, :]

def attend_head(operands):
    head_queries, head_keys, head_values, head_context_keys, head_context_values, lift = operands
    tokens = head_queries.shape[0]
    group = head_queries.shape[1]
    block = math.gcd(tokens, 512)
    keys_wide = head_keys.astype(jnp.float32)
    values_wide = head_values.astype(jnp.float32)
    context_keys_wide = head_context_keys.astype(jnp.float32)
    context_values_wide = head_context_values.astype(jnp.float32)

    def one_block(query_block):
        query_wide = query_block.astype(jnp.float32)
        latent_scores = jnp.einsum('qgd,sd->gqs', query_wide, keys_wide) * HEAD ** (-0.5)
        context_scores = jnp.einsum('qgd,sd->gqs', query_wide, context_keys_wide) * HEAD ** (-0.5) + lift[:, None, None]
        top = jnp.maximum(lax.optimization_barrier(jnp.max(latent_scores, axis=-1)), lax.optimization_barrier(jnp.max(context_scores, axis=-1)))[..., None]
        latent_weights = jnp.exp(latent_scores - top)
        context_weights = jnp.exp(context_scores - top)
        total = lax.optimization_barrier(jnp.sum(latent_weights, axis=-1)) + lax.optimization_barrier(jnp.sum(context_weights, axis=-1))
        summed = jnp.einsum('gqs,sd->qgd', latent_weights.astype(jnp.bfloat16).astype(jnp.float32), values_wide)
        summed = summed + jnp.einsum('gqs,sd->qgd', context_weights.astype(jnp.bfloat16).astype(jnp.float32), context_values_wide)
        return (summed / jnp.transpose(total)[:, :, None]).astype(jnp.bfloat16)
    result = lax.map(one_block, head_queries.reshape(tokens // block, block, group, HEAD))
    return result.reshape(tokens, group, HEAD)

def reference(latent, context, conditioning, context_conditioning, shift_weight, scale_weight, gate_weight, norm_gain, query_weight, key_weight, value_weight, query_gain, key_gain, context_lift, output_weight):
    signals = jnp.stack([jax.nn.silu(conditioning), jax.nn.silu(context_conditioning)]).astype(jnp.bfloat16)
    shifts = jnp.dot(signals, shift_weight, preferred_element_type=jnp.float32)
    scales = jnp.dot(signals, scale_weight, preferred_element_type=jnp.float32)
    gate = jnp.dot(signals[0:1], gate_weight, preferred_element_type=jnp.float32)[0]
    hidden = (normalize(latent.astype(jnp.float32), norm_gain) * (1.0 + scales[0]) + shifts[0]).astype(jnp.bfloat16)
    context_hidden = (normalize(context.astype(jnp.float32), norm_gain) * (1.0 + scales[1]) + shifts[1]).astype(jnp.bfloat16)
    tokens = latent.shape[0]
    group = Q_HEADS // KV_HEADS
    cos_table, sin_table = rotary_tables(0, tokens)
    raw_queries = jnp.dot(hidden, query_weight, preferred_element_type=jnp.float32).reshape(tokens, Q_HEADS, HEAD)
    queries = rotate(normalize(raw_queries, query_gain), cos_table, sin_table).astype(jnp.bfloat16)
    raw_keys = jnp.dot(hidden, key_weight, preferred_element_type=jnp.float32).reshape(tokens, KV_HEADS, HEAD)
    keys = rotate(normalize(raw_keys, key_gain), cos_table, sin_table).astype(jnp.bfloat16)
    values = jnp.dot(hidden, value_weight, preferred_element_type=jnp.float32).astype(jnp.bfloat16).reshape(tokens, KV_HEADS, HEAD)
    raw_context_keys = jnp.dot(context_hidden, key_weight, preferred_element_type=jnp.float32).reshape(CTX, KV_HEADS, HEAD)
    context_keys = normalize(raw_context_keys, key_gain).astype(jnp.bfloat16)
    context_values = jnp.dot(context_hidden, value_weight, preferred_element_type=jnp.float32).astype(jnp.bfloat16).reshape(CTX, KV_HEADS, HEAD)
    operands = (jnp.transpose(queries.reshape(tokens, KV_HEADS, group, HEAD), (1, 0, 2, 3)), jnp.transpose(keys, (1, 0, 2)), jnp.transpose(values, (1, 0, 2)), jnp.transpose(context_keys, (1, 0, 2)), jnp.transpose(context_values, (1, 0, 2)), context_lift.reshape(KV_HEADS, group))
    attended = lax.map(attend_head, operands)
    attended = jnp.transpose(attended, (1, 0, 2, 3)).reshape(tokens, Q_HEADS * HEAD)
    projection = jnp.dot(attended, output_weight, preferred_element_type=jnp.float32)
    return (latent.astype(jnp.float32) + gate * projection).astype(jnp.bfloat16)
```

```python
import functools
import math

import jax
import jax.numpy as jnp
from jax import lax
from jax.experimental import pallas as pl
from jax.experimental.pallas import tpu as pltpu
from jax.sharding import PartitionSpec as P

HEAD = 64
GRID = 64
TILE = 128
EPSILON = 1e-06
ROTARY_BASE = 10000.0
LOG2E = math.log2(math.e)
F32 = jnp.float32
BF16 = jnp.bfloat16


NT = (((1,), (1,)), ((), ()))


def dot(a, b):
    return jnp.dot(a, b, preferred_element_type=F32)


def cost(flops, nbytes):
    return pl.CostEstimate(flops=int(flops), bytes_accessed=int(nbytes), transcendentals=0)


def swap(value, axis, size, mask):
    return lax.ppermute(value, axis, [(i, i ^ mask) for i in range(size)])


def modulation_kernel(cond, ccond, shift, scale, gate, out):
    def signal(ref):
        v = ref[...]
        return (v / (1.0 + jnp.exp(-v))).astype(BF16)

    both = jnp.concatenate([signal(cond), signal(ccond)], axis=0)
    both = jnp.concatenate([both, jnp.zeros((6,) + both.shape[1:], F32).astype(BF16)], axis=0)
    s = dot(both, shift[...])
    c = dot(both, scale[...])
    g = dot(both, gate[...])
    out[0:1, :] = s[0:1]
    out[1:2, :] = c[0:1]
    out[2:3, :] = g[0:1]
    out[3:4, :] = s[1:2]
    out[4:5, :] = c[1:2]
    out[5:8, :] = jnp.zeros((3, out.shape[1]), F32)


def modulation_partial(cond, ccond, shift, scale, gate):
    width = shift.shape[1]
    depth = cond.shape[0]
    return pl.pallas_call(
        modulation_kernel,
        out_shape=jax.ShapeDtypeStruct((8, width), F32),
        cost_estimate=cost(6 * 8 * depth * width, 6 * depth * width),
        name="modulation",
    )(cond.reshape(1, depth), ccond.reshape(1, depth), shift, scale, gate)


def head_scale(x):
    width = x.shape[1]
    square = x * x
    high = square.astype(BF16)
    low = (square - high.astype(F32)).astype(BF16)
    rows = lax.broadcasted_iota(jnp.int32, (width, width), 0) // HEAD
    cols = lax.broadcasted_iota(jnp.int32, (width, width), 1) // HEAD
    ones = jnp.where(rows == cols, 1.0, 0.0).astype(BF16)
    mean = (dot(high, ones) + dot(low, ones)) * (1.0 / HEAD)
    return lax.rsqrt(mean + EPSILON)


def turn(x, tables):
    width = x.shape[1]
    left = pltpu.roll(x, width - 1, 1)
    right = pltpu.roll(x, 1, 1)
    return x * tables[0] + left * tables[1] + right * tables[2]


def pieces_of(x, width):
    return [x[:, i : i + width] for i in range(0, x.shape[1], width)]


def finish_heads(x, gain, tables):
    out = []
    step = TILE if x.shape[1] % TILE == 0 else HEAD
    tables = [t[:, :step] for t in tables]
    gain = gain[:, :step]
    for part in pieces_of(x, step):
        out.append(turn(part * head_scale(part) * gain, tables))
    return [h for part in out for h in pieces_of(part, HEAD)]


def modulate(x, gain, scale, shift, dest, row):
    rows = x.shape[0]
    x = x.astype(F32)
    inverse = lax.rsqrt(jnp.mean(x * x, axis=1, keepdims=True) + EPSILON)
    dest[row : row + rows, :] = (x * inverse * gain * (1.0 + scale) + shift).astype(BF16)


def kv_kernel(count, *refs):
    pieces = refs[:count]
    context, mod, norm_gain, key_weight, value_weight, key_gain, cos, sin_e, sin_o = refs[count : count + 9]
    hidden, packed = refs[count + 9 :]
    parts = mod.shape[0] // 8

    def vector(index):
        return jnp.concatenate([mod[8 * t + index : 8 * t + index + 1, :] for t in range(parts)], axis=1)

    gain = norm_gain[...]
    shift, scale, cshift, cscale = vector(0), vector(1), vector(3), vector(4)
    row = 0
    for piece in pieces:
        modulate(piece[...], gain, scale, shift, hidden, row)
        row += piece.shape[0]
    modulate(context[...], gain, cscale, cshift, hidden, row)
    h = hidden[...]
    keys = dot(h, key_weight[...])
    values = dot(h, value_weight[...])
    tables = (cos[...], sin_e[...], sin_o[...])
    heads = finish_heads(keys, key_gain[...], tables)
    for k, key in enumerate(heads):
        packed[:, k * TILE : (k + 1) * TILE] = jnp.concatenate(
            [key, values[:, k * HEAD : (k + 1) * HEAD]], axis=1
        ).astype(BF16)


def keys_values(pieces, context, mod, norm_gain, key_weight, value_weight, key_gain, tables):
    rows = sum(p.shape[0] for p in pieces) + context.shape[0]
    depth = context.shape[1]
    width = key_weight.shape[1]
    return pl.pallas_call(
        functools.partial(kv_kernel, len(pieces)),
        out_shape=(
            jax.ShapeDtypeStruct((rows, depth), BF16),
            jax.ShapeDtypeStruct((rows, 2 * width), BF16),
        ),
        cost_estimate=cost(4 * rows * depth * width, 4 * rows * depth + 4 * depth * width),
        name="keys_values",
    )(*pieces, context, mod, norm_gain, key_weight, value_weight, key_gain, *tables)


def query_kernel(hidden, weight, gain, cos, sin_e, sin_o, out):
    x = dot(hidden[...], weight[...])
    heads = finish_heads(x, gain[...], (cos[...], sin_e[...], sin_o[...]))
    for i, head in enumerate(heads):
        head = (head * (HEAD**-0.5)).astype(BF16)
        out[i] = jnp.concatenate([head, jnp.zeros_like(head)], axis=1)


def queries_of(hidden, weight, gain, tables, rows):
    depth, width = weight.shape
    step = min(width, 2 * TILE)
    heads = step // HEAD
    table = pl.BlockSpec((rows, TILE), lambda i: (0, 0))
    return pl.pallas_call(
        query_kernel,
        grid=(width // step,),
        in_specs=[
            pl.BlockSpec((rows, depth), lambda i: (0, 0)),
            pl.BlockSpec((depth, step), lambda i: (0, i)),
            pl.BlockSpec((1, TILE), lambda i: (0, 0)),
            table,
            table,
            table,
        ],
        out_specs=pl.BlockSpec((heads, rows, TILE), lambda i: (i, 0, 0)),
        out_shape=jax.ShapeDtypeStruct((width // HEAD, rows, TILE), BF16),
        cost_estimate=cost(2 * rows * depth * width, 2 * rows * depth + 2 * depth * width),
        name="queries",
    )(hidden, weight, gain, *tables)


def attention_kernel(n_blocks, n_context, has_state, final, group, chunk, *refs):
    refs = list(refs)
    q_ref = refs.pop(0)
    blocks = [refs.pop(0) for _ in range(n_blocks)]
    contexts = [refs.pop(0) for _ in range(n_context)]
    lift = refs.pop(0) if n_context else None
    state = refs.pop(0) if has_state else None
    outs = refs
    head = pl.program_id(0)
    kv = [b[...] for b in blocks]
    if n_context:
        kv.append(jnp.concatenate([c[...] for c in contexts], axis=0))
    lane = lax.broadcasted_iota(jnp.int32, (1, TILE), 1)
    vh = [jnp.where(lane < HEAD, jnp.ones((), BF16), b) for b in kv]
    rows = q_ref.shape[1]

    work = [(g, r) for r in range(0, rows, chunk) for g in range(group)]

    def scores(item):
        g, r = item
        q = q_ref[g, r : r + chunk, :]
        return [lax.dot_general(q, b, NT, preferred_element_type=F32) for b in kv]

    def absorb(item, s):
        g, r = item
        s = [x * LOG2E for x in s]
        if n_context:
            s[-1] = s[-1] + lift[head * group + g] * LOG2E
        top = functools.reduce(jnp.maximum, [jnp.max(x, axis=1, keepdims=True) for x in s])
        if has_state:
            old = state[g, r : r + chunk, :]
            before = old[:, 0:1]
            top = jnp.maximum(top, before)
        total = None
        for x, v in zip(s, vh):
            term = dot(jnp.exp2(x - top).astype(BF16), v)
            total = term if total is None else total + term
        if has_state:
            total = total + old * jnp.exp2(before - top)
        return top, total

    done = {}
    ahead = scores(work[0])
    for i, item in enumerate(work):
        s = ahead
        if i + 1 < len(work):
            ahead = scores(work[i + 1])
        top, total = absorb(item, s)
        g, r = item
        if not final:
            outs[0][g, r : r + chunk, :] = jnp.where(lane < HEAD // 2, top, total)
        else:
            value = total / total[:, HEAD // 2 : HEAD // 2 + 1]
            done[g] = value[:, HEAD:]
            if g == group - 1:
                whole = jnp.concatenate([done[j] for j in range(group)], axis=1).astype(BF16)
                size = outs[0].shape[0]
                for j in range(0, chunk, size):
                    outs[(r + j) // size][...] = whole[j : j + size]


def attention(queries, blocks, contexts, lift, state, group, length, pieces):
    heads, rows, _ = queries.shape
    kv_heads = heads // group
    chunk = min(rows, 256)
    final = pieces > 0
    in_specs = [pl.BlockSpec((group, rows, TILE), lambda k: (k, 0, 0))]
    args = [queries]
    keys = 0
    for array, size, first in list(blocks) + list(contexts):
        in_specs.append(pl.BlockSpec((size, TILE), lambda k, first=first: (first, k)))
        args.append(array)
        keys += size
    if contexts:
        in_specs.append(pl.BlockSpec(memory_space=pltpu.SMEM))
        args.append(lift)
    state_spec = pl.BlockSpec((group, rows, TILE), lambda k: (k, 0, 0))
    if state is not None:
        in_specs.append(state_spec)
        args.append(state)
    if final:
        out_shape = [jax.ShapeDtypeStruct((rows // pieces, heads * HEAD), BF16)] * pieces
        out_specs = [pl.BlockSpec((rows // pieces, group * HEAD), lambda k: (0, k))] * pieces
    else:
        out_shape = jax.ShapeDtypeStruct((heads, rows, TILE), F32)
        out_specs = state_spec
    return pl.pallas_call(
        functools.partial(
            attention_kernel, len(blocks), len(contexts), state is not None, final, group, chunk
        ),
        grid=(kv_heads,),
        in_specs=in_specs,
        out_specs=out_specs,
        out_shape=out_shape,
        cost_estimate=cost(16 * heads * rows * keys * HEAD, 4 * heads * rows * TILE),
        name="attention",
    )(*args)


def output_kernel(count, *refs):
    attended = refs[:count]
    weights = refs[count : 2 * count]
    latent, mod, out = refs[2 * count :]
    total = None
    for a, w in zip(attended, weights):
        term = dot(a[...], w[...])
        total = term if total is None else total + term
    out[...] = (latent[...].astype(F32) + mod[2:3, :] * total).astype(BF16)


def project(attended, weights, latent, mod):
    count = len(attended)
    rows, depth = latent.shape
    inner = attended[0].shape[1]
    step = mod.shape[1]
    return pl.pallas_call(
        functools.partial(output_kernel, count),
        grid=(depth // step,),
        in_specs=[pl.BlockSpec((rows, inner), lambda i: (0, 0))] * count
        + [pl.BlockSpec((inner, step), lambda i: (0, i))] * count
        + [
            pl.BlockSpec((rows, step), lambda i: (0, i)),
            pl.BlockSpec((8, step), lambda i: (i, 0)),
        ],
        out_specs=pl.BlockSpec((rows, step), lambda i: (0, i)),
        out_shape=jax.ShapeDtypeStruct((rows, depth), BF16),
        cost_estimate=cost(2 * rows * depth * inner * count, 2 * depth * inner * count),
        name="output",
    )(*attended, *weights, latent, mod)


def rotary_tables(rank, tp, rows, context_rows):
    piece = jnp.arange(tp * rows, dtype=jnp.int32) // rows
    inside = jnp.arange(tp * rows, dtype=jnp.int32) % rows
    position = (rank // tp * tp + jnp.bitwise_xor(rank % tp, piece)) * rows + inside
    quarter = HEAD // 4
    frequency = ROTARY_BASE ** (-jnp.arange(quarter, dtype=F32) / quarter)
    lane = jnp.arange(TILE, dtype=jnp.int32)
    pair = lane % HEAD // 2
    axis = jnp.where(
        (pair < quarter)[None, :],
        (position // GRID).astype(F32)[:, None],
        (position % GRID).astype(F32)[:, None],
    )
    angle = axis * frequency[pair % quarter][None, :]
    sine = jnp.sin(angle)
    even = (lane % 2 == 0)[None, :]
    still = jnp.zeros((context_rows, TILE), F32)
    return (
        jnp.concatenate([jnp.cos(angle), still + 1.0]),
        jnp.concatenate([jnp.where(even, -sine, 0.0), still]),
        jnp.concatenate([jnp.where(even, 0.0, sine), still]),
    )


def shards(
    sp,
    tp,
    latent,
    context,
    conditioning,
    context_conditioning,
    shift_weight,
    scale_weight,
    gate_weight,
    norm_gain,
    query_weight,
    key_weight,
    value_weight,
    query_gain,
    key_gain,
    context_lift,
    output_weight,
):
    rows = latent.shape[0]
    length = rows * tp
    context_rows = context.shape[0]
    group = query_weight.shape[1] // key_weight.shape[1]
    tp_bits = [1 << b for b in reversed(range(tp.bit_length() - 1))]

    def gather(value):
        have = {0: value}
        for bit in tp_bits:
            have.update({j | bit: swap(v, "tp", tp, bit) for j, v in list(have.items())})
        return [have[j] for j in range(tp)]

    pieces = gather(latent)

    partial = modulation_partial(
        conditioning, context_conditioning, shift_weight, scale_weight, gate_weight
    )
    bits = [1 << b for b in range(sp.bit_length() - 1)]
    for i in range(0, len(bits), 2):
        pair = bits[i : i + 2]
        masks = pair + [sum(pair)] if len(pair) == 2 else pair
        partial = sum([swap(partial, "sp", sp, m) for m in masks], partial)
    mod = lax.all_gather(partial, "tp", axis=0, tiled=True)

    rank = lax.axis_index("sp") * tp + lax.axis_index("tp")
    tables = rotary_tables(rank, tp, rows, context_rows)
    key_tile = jnp.tile(key_gain, TILE // HEAD).reshape(1, TILE)
    query_tile = jnp.tile(query_gain, TILE // HEAD).reshape(1, TILE)

    hidden, packed = keys_values(
        pieces, context, mod, norm_gain.reshape(1, -1), key_weight, value_weight, key_tile, tables
    )

    order = list(range(0, sp, 2)) + list(range(sp - 1, 0, -2))
    ahead = [(order[i], order[(i + 1) % sp]) for i in range(sp)]
    back = [(b, a) for a, b in ahead]
    across = [(order[i], order[(i + sp // 2) % sp]) for i in range(sp)]
    far_context = lax.ppermute(packed[length:], "sp", across)
    contexts = [(packed, context_rows, length // context_rows), (far_context, context_rows, 0)]
    queries = queries_of(hidden, query_weight, query_tile, tables, length)

    output_weight, packed = lax.optimization_barrier((output_weight, packed))
    up, down = packed, packed
    waiting = [(packed, length, 0)]
    state = None
    for step in range(1, sp // 2):
        up = lax.ppermute(up, "sp", ahead)
        down = lax.ppermute(down, "sp", back)
        state = attention(queries, waiting, [], None, state, group, length, 0)
        waiting = [(up, length, 0), (down, length, 0)]
        contexts += [(b, context_rows, length // context_rows) for b in (up, down)]
    half = length // 2
    up = lax.ppermute(up[:half], "sp", ahead)
    down = lax.ppermute(down[half:length], "sp", back)
    state = attention(queries, waiting, contexts, context_lift, state, group, length, 0)
    weights = gather(output_weight)
    attended = attention(
        queries, [(up, half, 0), (down, half, 0)], [], None, state, group, length, tp
    )
    attended = list(attended)
    for bit in tp_bits:
        attended = [swap(a, "tp", tp, bit) if j & bit else a for j, a in enumerate(attended)]
    return project(attended, weights, latent, mod)


def solution(mesh):
    in_specs = (
        P(("sp", "tp"), None),
        P("sp", None),
        P("sp"),
        P("sp"),
        P("sp", "tp"),
        P("sp", "tp"),
        P("sp", "tp"),
        P(),
        P(None, "tp"),
        P(None, "tp"),
        P(None, "tp"),
        P(),
        P(),
        P("tp"),
        P("tp", None),
    )
    return jax.shard_map(
        functools.partial(shards, mesh.shape["sp"], mesh.shape["tp"]),
        mesh=mesh,
        in_specs=in_specs,
        out_specs=P(("sp", "tp"), None),
        check_vma=False,
    )
```

```python
import functools

import jax
import jax.numpy as jnp
from jax import lax
from jax.experimental import pallas as pl
from jax.experimental.pallas import tpu as pltpu
from jax.sharding import PartitionSpec as P


HEAD = 64
GRID = 64
TILE = 128
EPSILON = 1e-06
ROTARY_BASE = 10000.0
F32 = jnp.float32
BF16 = jnp.bfloat16


VMEM_LIMIT = 20 << 20
IN_VMEM = pl.BlockSpec(memory_space=pltpu.VMEM)

NT = (((1,), (1,)), ((), ()))


def dot(a, b):
    return jnp.dot(a, b, preferred_element_type=F32)


def cost(flops, nbytes):
    return pl.CostEstimate(flops=int(flops), bytes_accessed=int(nbytes), transcendentals=0)


def swap(value, axis, size, mask):
    return lax.ppermute(value, axis, [(i, i ^ mask) for i in range(size)])


def modulation_kernel(cond, ccond, shift, scale, gate, out):
    def signal(ref):
        v = ref[...]
        return (v / (1.0 + jnp.exp(-v))).astype(BF16)

    both = jnp.concatenate([signal(cond), signal(ccond)], axis=0)
    both = jnp.concatenate([both, jnp.zeros((6,) + both.shape[1:], F32).astype(BF16)], axis=0)
    s = dot(both, shift[...])
    c = dot(both, scale[...])
    g = dot(both, gate[...])
    out[0:1, :] = s[0:1]
    out[1:2, :] = c[0:1]
    out[2:3, :] = g[0:1]
    out[3:4, :] = s[1:2]
    out[4:5, :] = c[1:2]
    out[5:8, :] = jnp.zeros((3, out.shape[1]), F32)


def modulation_partial(cond, ccond, shift, scale, gate):
    width = shift.shape[1]
    depth = cond.shape[0]
    return pl.pallas_call(
        modulation_kernel,
        out_shape=jax.ShapeDtypeStruct((8, width), F32),
        cost_estimate=cost(6 * 8 * depth * width, 6 * depth * width),
        name="modulation",
    )(cond.reshape(1, depth), ccond.reshape(1, depth), shift, scale, gate)


def head_scale(x):
    width = x.shape[1]
    square = x * x
    high = square.astype(BF16)
    low = (square - high.astype(F32)).astype(BF16)
    rows = lax.broadcasted_iota(jnp.int32, (width, width), 0) // HEAD
    cols = lax.broadcasted_iota(jnp.int32, (width, width), 1) // HEAD
    ones = jnp.where(rows == cols, 1.0, 0.0).astype(BF16)
    mean = (dot(high, ones) + dot(low, ones)) * (1.0 / HEAD)
    return lax.rsqrt(mean + EPSILON)


def turn(x, tables):
    width = x.shape[1]
    left = pltpu.roll(x, width - 1, 1)
    right = pltpu.roll(x, 1, 1)
    return x * tables[0] + left * tables[1] + right * tables[2]


def pieces_of(x, width):
    return [x[:, i : i + width] for i in range(0, x.shape[1], width)]


def finish_heads(x, gain, tables):
    out = []
    step = TILE if x.shape[1] % TILE == 0 else HEAD
    tables = [t[:, :step] for t in tables]
    gain = jnp.concatenate([gain] * (step // HEAD), axis=1)
    for part in pieces_of(x, step):
        out.append(turn(part * head_scale(part) * gain, tables))
    return [h for part in out for h in pieces_of(part, HEAD)]


def modulate(x, gain, shift, dest, row):
    rows = x.shape[0]
    x = x.astype(F32)
    inverse = lax.rsqrt(jnp.mean(x * x, axis=1, keepdims=True) + EPSILON)
    dest[row : row + rows, :] = (x * inverse * gain + shift).astype(BF16)


def kv_kernel(count, *refs):
    pieces = refs[:count]
    context, mod, gains, weight, cos, sin_e, sin_o = refs[count : count + 7]
    hidden, packed = refs[count + 7 :]
    norm_gain = gains[:, : context.shape[1]]
    key_gain = gains[:, context.shape[1] : context.shape[1] + HEAD]
    parts = mod.shape[0] // 8

    def vector(index):
        return jnp.concatenate([mod[8 * t + index : 8 * t + index + 1, :] for t in range(parts)], axis=1)

    gain = norm_gain * (1.0 + vector(1))
    shift = vector(0)
    row = 0
    for piece in pieces:
        modulate(piece[...], gain, shift, hidden, row)
        row += piece.shape[0]
    modulate(context[...], norm_gain * (1.0 + vector(4)), vector(3), hidden, row)
    h = hidden[...]
    width = weight.shape[1] // 2
    keys = dot(h, weight[:, :width])
    values = dot(h, weight[:, width:])
    tables = (cos[...], sin_e[...], sin_o[...])
    heads = finish_heads(keys, key_gain, tables)
    for k, key in enumerate(heads):
        packed[:, k * TILE : (k + 1) * TILE] = jnp.concatenate(
            [key, values[:, k * HEAD : (k + 1) * HEAD]], axis=1
        ).astype(BF16)


def keys_values(pieces, context, mod, gains, weight, tables):
    rows = sum(p.shape[0] for p in pieces) + context.shape[0]
    depth = context.shape[1]
    width = weight.shape[1] // 2
    return pl.pallas_call(
        functools.partial(kv_kernel, len(pieces)),
        out_shape=(
            jax.ShapeDtypeStruct((rows, depth), BF16),
            jax.ShapeDtypeStruct((rows, 2 * width), BF16),
        ),
        in_specs=[IN_VMEM] * (len(pieces) + 7),
        out_specs=(IN_VMEM, IN_VMEM),
        compiler_params=pltpu.CompilerParams(vmem_limit_bytes=VMEM_LIMIT),
        cost_estimate=cost(4 * rows * depth * width, 4 * rows * depth + 4 * depth * width),
        name="keys_values",
    )(*pieces, context, mod, gains, weight, *tables)


def query_kernel(hidden, weight, gains, cos, sin_e, sin_o, out):
    rows = out.shape[1]
    tables = (cos[0:rows, :], sin_e[0:rows, :], sin_o[0:rows, :])
    width = weight.shape[1]
    gain = gains[:, hidden.shape[1] + HEAD :]
    step = min(width, 2 * TILE)
    for start in range(0, width, step):
        x = dot(hidden[0:rows, :], weight[:, start : start + step])
        for i, head in enumerate(finish_heads(x, gain, tables)):
            head = (head * (HEAD**-0.5)).astype(BF16)
            out[start // HEAD + i] = jnp.concatenate([head, jnp.zeros_like(head)], axis=1)


def queries_of(hidden, weight, gains, tables, rows):
    depth, width = weight.shape
    return pl.pallas_call(
        query_kernel,
        in_specs=[IN_VMEM] * 6,
        out_specs=IN_VMEM,
        out_shape=jax.ShapeDtypeStruct((width // HEAD, rows, TILE), BF16),
        compiler_params=pltpu.CompilerParams(vmem_limit_bytes=VMEM_LIMIT),
        cost_estimate=cost(2 * rows * depth * width, 2 * rows * depth + 2 * depth * width),
        name="queries",
    )(hidden, weight, gains, *tables)


STATE = HEAD + 16


def attention_kernel(spans, lifted, has_state, final, group, chunk, *refs):
    refs = list(refs)
    q_ref = refs.pop(0)
    blocks = [refs.pop(0) for _ in spans]
    lift = refs.pop(0) if lifted else None
    state = refs.pop(0) if has_state else None
    value_rows, held = refs[-3], refs[-2:]
    outs = refs[:-3]
    rows = q_ref.shape[1]
    kv_heads = q_ref.shape[0] // group
    sizes = [end - first for first, _, end in spans]
    starts = [sum(sizes[:i]) for i in range(len(sizes))]
    plain = [(st, middle - first) for st, (first, middle, _) in zip(starts, spans) if middle > first]
    raised = [
        (st + middle - first, end - middle)
        for st, (first, middle, end) in zip(starts, spans)
        if end > middle
    ]

    def tile(ref, span, k):
        return ref[span[0] : span[2], pl.ds(pl.multiple_of(k * TILE, TILE), TILE)]

    for k in range(kv_heads):
        for ref, span, start, size in zip(blocks, spans, starts, sizes):
            value_rows[k, 0:HEAD, start : start + size] = tile(ref, span, k).T[HEAD:]
            value_rows[k, HEAD:, start : start + size] = jnp.ones((16, size), BF16)

    work = [(g, r) for r in range(0, rows, chunk) for g in range(group)]

    def scores(k, item, slot):
        g, r = item
        q = q_ref[k * group + g, r : r + chunk, :]
        for ref, span, start, size in zip(blocks, spans, starts, sizes):
            held[slot][start : start + size, :] = lax.dot_general(
                tile(ref, span, k), q, NT, preferred_element_type=F32
            )

    def absorb(k, item, slot):
        g, r = item
        h = k * group + g
        parts = [(st, held[slot][st : st + n, :]) for st, n in plain]
        parts += [(st, held[slot][st : st + n, :] + lift[h]) for st, n in raised]
        top = functools.reduce(
            jnp.maximum, [jnp.max(x, axis=0, keepdims=True) for _, x in parts]
        )
        if has_state:
            before = state[h, HEAD + 8 : HEAD + 9, r : r + chunk]
            top = jnp.maximum(top, before)
        parts.sort(key=lambda part: part[0])
        weights = jnp.concatenate([jnp.exp(x - top).astype(BF16) for _, x in parts], axis=0)
        total = dot(value_rows[k], weights)
        if has_state:
            total = total + state[h, :, r : r + chunk] * jnp.exp(before - top)
        if not final:
            outs[0][h, 0 : HEAD + 8, r : r + chunk] = total[: HEAD + 8]
            outs[0][h, HEAD + 8 :, r : r + chunk] = jnp.broadcast_to(top, (8, chunk))
            return None
        return total[:HEAD] / total[HEAD : HEAD + 1]

    scores(0, work[0], 0)

    @pl.loop(0, kv_heads)
    def _(k):
        done = {}
        for i, item in enumerate(work):
            if i + 1 < len(work):
                scores(k, work[i + 1], (i + 1) % 2)
            else:
                scores(jnp.minimum(k + 1, kv_heads - 1), work[0], (i + 1) % 2)
            g, r = item
            done[g] = absorb(k, item, i % 2)
            if final and g == group - 1:
                whole = jnp.concatenate([done[j] for j in range(group)], axis=0).T.astype(BF16)
                size = outs[0].shape[0]
                width = group * HEAD
                lanes = pl.ds(pl.multiple_of(k * width, width), width)
                for j in range(0, chunk, size):
                    outs[(r + j) // size][:, lanes] = whole[j : j + size]


def attention(queries, blocks, lift, state, group, pieces):
    heads, rows, _ = queries.shape
    kv_heads = heads // group
    chunk = min(rows, 256)
    final = pieces > 0
    spans = [b[1:] for b in blocks]
    keys = sum(end - first for first, _, end in spans)
    lifted = any(end > middle for _, middle, end in spans)
    args = [queries] + [b[0] for b in blocks]
    in_specs = [IN_VMEM] * len(args)
    if lifted:
        in_specs.append(pl.BlockSpec(memory_space=pltpu.SMEM))
        args.append(lift)
    if state is not None:
        in_specs.append(IN_VMEM)
        args.append(state)
    if final:
        out_shape = [jax.ShapeDtypeStruct((rows // pieces, heads * HEAD), BF16)] * pieces
    else:
        out_shape = [jax.ShapeDtypeStruct((heads, STATE, rows), F32)]
    out = pl.pallas_call(
        functools.partial(
            attention_kernel, spans, lifted, state is not None, final, group, chunk
        ),
        in_specs=in_specs,
        out_specs=[IN_VMEM] * len(out_shape),
        out_shape=out_shape,
        scratch_shapes=[
            pltpu.VMEM((kv_heads, STATE, keys), BF16),
            pltpu.VMEM((keys, chunk), F32),
            pltpu.VMEM((keys, chunk), F32),
        ],
        compiler_params=pltpu.CompilerParams(vmem_limit_bytes=VMEM_LIMIT),
        cost_estimate=cost(16 * heads * rows * keys * HEAD, 4 * heads * rows * TILE),
        name="attention",
    )(*args)
    return list(out) if final else out[0]


def output_kernel(count, *refs):
    attended = refs[:count]
    weights = refs[count : 2 * count]
    latent, mod, out = refs[2 * count :]
    step = mod.shape[1]
    for i in range(out.shape[1] // step):
        total = None
        for a, w in zip(attended, weights):
            term = dot(a[...], w[:, i * step : (i + 1) * step])
            total = term if total is None else total + term
        gate = mod[8 * i + 2 : 8 * i + 3, :]
        old = latent[:, i * step : (i + 1) * step].astype(F32)
        out[:, i * step : (i + 1) * step] = (old + gate * total).astype(BF16)


def project(attended, weights, latent, mod):
    count = len(attended)
    rows, depth = latent.shape
    inner = attended[0].shape[1]
    return pl.pallas_call(
        functools.partial(output_kernel, count),
        in_specs=[IN_VMEM] * (2 * count + 2),
        out_specs=IN_VMEM,
        out_shape=jax.ShapeDtypeStruct((rows, depth), BF16),
        compiler_params=pltpu.CompilerParams(vmem_limit_bytes=VMEM_LIMIT),
        cost_estimate=cost(2 * rows * depth * inner * count, 2 * depth * inner * count),
        name="output",
    )(*attended, *weights, latent, mod)


def rotary_tables(rank, tp, rows, context_rows):
    index = lax.broadcasted_iota(jnp.int32, (tp * rows + context_rows, TILE), 0)
    lane = lax.broadcasted_iota(jnp.int32, (tp * rows + context_rows, TILE), 1)
    piece = index // rows
    position = (rank // tp * tp + jnp.bitwise_xor(rank % tp, piece)) * rows + index % rows
    quarter = HEAD // 4
    pair = lane % HEAD // 2
    frequency = ROTARY_BASE ** (-(pair % quarter).astype(F32) / quarter)
    place = jnp.where(pair < quarter, position // GRID, position % GRID).astype(F32)
    angle = jnp.where(index < tp * rows, place, 0.0) * frequency
    sine = jnp.sin(angle)
    even = lane % 2 == 0
    return jnp.cos(angle), jnp.where(even, -sine, 0.0), jnp.where(even, 0.0, sine)


def shards(
    sp,
    tp,
    latent,
    context,
    conditioning,
    context_conditioning,
    shift_weight,
    scale_weight,
    gate_weight,
    norm_gain,
    query_weight,
    key_weight,
    value_weight,
    query_gain,
    key_gain,
    context_lift,
    output_weight,
):
    rows = latent.shape[0]
    length = rows * tp
    context_rows = context.shape[0]
    group = query_weight.shape[1] // key_weight.shape[1]
    tp_bits = [1 << b for b in reversed(range(tp.bit_length() - 1))]

    def spread(have, bit):
        have.update({j | bit: swap(v, "tp", tp, bit) for j, v in list(have.items())})

    def tie(*values):
        return lax.optimization_barrier(values)

    pieces = {0: latent}
    spread(pieces, tp_bits[0])
    partial = modulation_partial(
        conditioning, context_conditioning, shift_weight, scale_weight, gate_weight
    )
    rank = lax.axis_index("sp") * tp + lax.axis_index("tp")
    gains = [v.reshape(1, -1) for v in (norm_gain, key_gain, query_gain)]
    early = [
        (*rotary_tables(rank, tp, rows, context_rows), jnp.concatenate(gains, axis=1)),
        (jnp.concatenate([key_weight, value_weight], axis=1),),
    ]
    ready = []
    bits = [1 << b for b in range(sp.bit_length() - 1)]
    for i in range(0, len(bits), 2):
        pair = bits[i : i + 2]
        masks = pair + [sum(pair)] if len(pair) == 2 else pair
        arrived = [swap(partial, "sp", sp, m) for m in masks]
        extra = early.pop(0) if early else ()
        tied = tie(*arrived, *extra)
        partial = sum(tied[: len(arrived)], partial)
        ready += tied[len(arrived) :]
    for extra in early:
        ready += extra
    *tables, gains, kv_weight = ready
    partial, pieces[tp_bits[0]] = tie(partial, pieces[tp_bits[0]])
    for bit in tp_bits[1:]:
        spread(pieces, bit)
    mod = lax.all_gather(partial, "tp", axis=0, tiled=True)

    hidden, packed = keys_values(
        [pieces[j] for j in range(tp)], context, mod, gains, kv_weight, tables
    )

    order = list(range(0, sp, 2)) + list(range(sp - 1, 0, -2))
    ahead = [(order[i], order[(i + 1) % sp]) for i in range(sp)]
    back = [(b, a) for a, b in ahead]
    across = [(order[i], order[(i + sp // 2) % sp]) for i in range(sp)]
    up, down = packed, packed
    waiting = [(packed, 0, length, length + context_rows)]
    state = None
    for step in range(1, sp // 2):
        up = lax.ppermute(up, "sp", ahead)
        down = lax.ppermute(down, "sp", back)
        if step == 1:
            queries = queries_of(hidden, query_weight, gains, tables, length)
            far_context = lax.ppermute(packed[length:], "sp", across)
            output_weight, _ = tie(output_weight, packed)
            weights = {0: output_weight}
            spread(weights, tp_bits[0])
        state = attention(queries, waiting, context_lift, state, group, 0)
        if step == 1:
            up, down, state, far_context = tie(up, down, state, far_context)
        else:
            up, down, state = tie(up, down, state)
        waiting = [(b, 0, length, length + context_rows) for b in (up, down)]
        if step == 2:
            waiting.append((far_context, 0, 0, context_rows))
    half = length // 2
    up = lax.ppermute(up[:half], "sp", ahead)
    down = lax.ppermute(down[half:length], "sp", back)
    state = attention(queries, waiting, context_lift, state, group, 0)
    first = tp_bits[0]
    up, down, state, weights[first] = tie(up, down, state, weights[first])
    for bit in tp_bits[1:]:
        spread(weights, bit)
    attended = attention(
        queries, [(up, 0, half, half), (down, 0, half, half)], context_lift, state, group, tp
    )
    for bit in tp_bits:
        attended = [swap(a, "tp", tp, bit) if j & bit else a for j, a in enumerate(attended)]
    return project(attended, [weights[j] for j in range(tp)], latent, mod)


def solution(mesh):
    in_specs = (
        P(("sp", "tp"), None),
        P("sp", None),
        P("sp"),
        P("sp"),
        P("sp", "tp"),
        P("sp", "tp"),
        P("sp", "tp"),
        P(),
        P(None, "tp"),
        P(None, "tp"),
        P(None, "tp"),
        P(),
        P(),
        P("tp"),
        P("tp", None),
    )
    return jax.shard_map(
        functools.partial(shards, mesh.shape["sp"], mesh.shape["tp"]),
        mesh=mesh,
        in_specs=in_specs,
        out_specs=P(("sp", "tp"), None),
        check_vma=False,
    )
```

```python
import functools

import jax
import jax.numpy as jnp
from jax import lax
from jax.experimental import pallas as pl
from jax.experimental.pallas import tpu as pltpu
from jax.sharding import PartitionSpec as P


HEAD = 64
GRID = 64
TILE = 128
EPSILON = 1e-06
ROTARY_BASE = 10000.0
F32 = jnp.float32
BF16 = jnp.bfloat16


VMEM_LIMIT = 20 << 20
IN_VMEM = pl.BlockSpec(memory_space=pltpu.VMEM)

NT = (((1,), (1,)), ((), ()))


def dot(a, b):
    return jnp.dot(a, b, preferred_element_type=F32)


def cost(flops, nbytes):
    return pl.CostEstimate(flops=int(flops), bytes_accessed=int(nbytes), transcendentals=0)


def swap(value, axis, size, mask):
    return lax.ppermute(value, axis, [(i, i ^ mask) for i in range(size)])


def modulation_kernel(cond, ccond, shift, scale, gate, out):
    def signal(ref):
        v = ref[...]
        return (v / (1.0 + jnp.exp(-v))).astype(BF16)

    both = jnp.concatenate([signal(cond), signal(ccond)], axis=0)
    both = jnp.concatenate([both, jnp.zeros((6,) + both.shape[1:], F32).astype(BF16)], axis=0)
    s = dot(both, shift[...])
    c = dot(both, scale[...])
    g = dot(both, gate[...])
    out[0:1, :] = s[0:1]
    out[1:2, :] = c[0:1]
    out[2:3, :] = g[0:1]
    out[3:4, :] = s[1:2]
    out[4:5, :] = c[1:2]
    out[5:8, :] = jnp.zeros((3, out.shape[1]), F32)


def modulation_partial(cond, ccond, shift, scale, gate):
    width = shift.shape[1]
    depth = cond.shape[0]
    return pl.pallas_call(
        modulation_kernel,
        out_shape=jax.ShapeDtypeStruct((8, width), F32),
        cost_estimate=cost(6 * 8 * depth * width, 6 * depth * width),
        name="modulation",
    )(cond.reshape(1, depth), ccond.reshape(1, depth), shift, scale, gate)


def head_scale(x):
    width = x.shape[1]
    square = x * x
    high = square.astype(BF16)
    low = (square - high.astype(F32)).astype(BF16)
    rows = lax.broadcasted_iota(jnp.int32, (width, width), 0) // HEAD
    cols = lax.broadcasted_iota(jnp.int32, (width, width), 1) // HEAD
    ones = jnp.where(rows == cols, 1.0, 0.0).astype(BF16)
    mean = (dot(high, ones) + dot(low, ones)) * (1.0 / HEAD)
    return lax.rsqrt(mean + EPSILON)


def turn(x, tables):
    width = x.shape[1]
    left = pltpu.roll(x, width - 1, 1)
    right = pltpu.roll(x, 1, 1)
    return x * tables[0] + left * tables[1] + right * tables[2]


def pieces_of(x, width):
    return [x[:, i : i + width] for i in range(0, x.shape[1], width)]


def finish_heads(x, gain, tables):
    out = []
    step = TILE if x.shape[1] % TILE == 0 else HEAD
    tables = [t[:, :step] for t in tables]
    gain = jnp.concatenate([gain] * (step // HEAD), axis=1)
    for part in pieces_of(x, step):
        out.append(turn(part * head_scale(part) * gain, tables))
    return [h for part in out for h in pieces_of(part, HEAD)]


def modulate(x, gain, shift, dest, row):
    rows = x.shape[0]
    x = x.astype(F32)
    inverse = lax.rsqrt(jnp.mean(x * x, axis=1, keepdims=True) + EPSILON)
    dest[row : row + rows, :] = (x * inverse * gain + shift).astype(BF16)


def kv_kernel(count, *refs):
    pieces = refs[:count]
    context, mod, gains, weight, cos, sin_e, sin_o = refs[count : count + 7]
    hidden, first, second = refs[count + 7 :]
    half = first.shape[0]
    norm_gain = gains[:, : context.shape[1]]
    key_gain = gains[:, context.shape[1] : context.shape[1] + HEAD]
    parts = mod.shape[0] // 8

    def vector(index):
        return jnp.concatenate([mod[8 * t + index : 8 * t + index + 1, :] for t in range(parts)], axis=1)

    gain = norm_gain * (1.0 + vector(1))
    shift = vector(0)
    row = 0
    for piece in pieces:
        modulate(piece[...], gain, shift, hidden, row)
        row += piece.shape[0]
    modulate(context[...], norm_gain * (1.0 + vector(4)), vector(3), hidden, row)
    h = hidden[...]
    width = weight.shape[1] // 2
    keys = dot(h, weight[:, :width])
    values = dot(h, weight[:, width:])
    tables = (cos[...], sin_e[...], sin_o[...])
    heads = finish_heads(keys, key_gain, tables)
    for k, key in enumerate(heads):
        tile = jnp.concatenate([key, values[:, k * HEAD : (k + 1) * HEAD]], axis=1).astype(BF16)
        first[:, k * TILE : (k + 1) * TILE] = tile[:half]
        second[:, k * TILE : (k + 1) * TILE] = tile[half:]


def keys_values(pieces, context, mod, gains, weight, tables):
    rows = sum(p.shape[0] for p in pieces) + context.shape[0]
    depth = context.shape[1]
    width = weight.shape[1] // 2
    half = (rows - context.shape[0]) // 2
    return pl.pallas_call(
        functools.partial(kv_kernel, len(pieces)),
        out_shape=(
            jax.ShapeDtypeStruct((rows, depth), BF16),
            jax.ShapeDtypeStruct((half, 2 * width), BF16),
            jax.ShapeDtypeStruct((rows - half, 2 * width), BF16),
        ),
        in_specs=[IN_VMEM] * (len(pieces) + 7),
        out_specs=(IN_VMEM, IN_VMEM, IN_VMEM),
        compiler_params=pltpu.CompilerParams(vmem_limit_bytes=VMEM_LIMIT),
        cost_estimate=cost(4 * rows * depth * width, 4 * rows * depth + 4 * depth * width),
        name="keys_values",
    )(*pieces, context, mod, gains, weight, *tables)


def query_kernel(hidden, weight, gains, cos, sin_e, sin_o, out):
    rows = out.shape[1]
    tables = (cos[0:rows, :], sin_e[0:rows, :], sin_o[0:rows, :])
    width = weight.shape[1]
    gain = gains[:, hidden.shape[1] + HEAD :]
    step = min(width, 2 * TILE)
    for start in range(0, width, step):
        x = dot(hidden[0:rows, :], weight[:, start : start + step])
        for i, head in enumerate(finish_heads(x, gain, tables)):
            head = (head * (HEAD**-0.5)).astype(BF16)
            out[start // HEAD + i] = jnp.concatenate([head, jnp.zeros_like(head)], axis=1)


def queries_of(hidden, weight, gains, tables, rows):
    depth, width = weight.shape
    return pl.pallas_call(
        query_kernel,
        in_specs=[IN_VMEM] * 6,
        out_specs=IN_VMEM,
        out_shape=jax.ShapeDtypeStruct((width // HEAD, rows, TILE), BF16),
        compiler_params=pltpu.CompilerParams(vmem_limit_bytes=VMEM_LIMIT),
        cost_estimate=cost(2 * rows * depth * width, 2 * rows * depth + 2 * depth * width),
        name="queries",
    )(hidden, weight, gains, *tables)


STATE = HEAD + 16


def attention_kernel(spans, lifted, has_state, final, group, chunk, window, unrolled, *refs):
    refs = list(refs)
    q_ref = refs.pop(0)
    blocks = [refs.pop(0) for _ in spans]
    lift = refs.pop(0) if lifted else None
    state = refs.pop(0) if has_state else None
    value_rows, held = refs[-3], refs[-2:]
    outs = refs[:-3]
    low, high = window
    kv_heads = q_ref.shape[0] // group
    sizes = [end - first for first, _, end in spans]
    starts = [sum(sizes[:i]) for i in range(len(sizes))]
    plain = [(st, middle - first) for st, (first, middle, _) in zip(starts, spans) if middle > first]
    raised = [
        (st + middle - first, end - middle)
        for st, (first, middle, end) in zip(starts, spans)
        if end > middle
    ]

    def aligned(k, width):
        return k * width if isinstance(k, int) else pl.multiple_of(k * width, width)

    def tile(ref, span, k):
        return ref[span[0] : span[2], pl.ds(aligned(k, TILE), TILE)]

    for k in range(kv_heads):
        for ref, span, start, size in zip(blocks, spans, starts, sizes):
            value_rows[k, 0:HEAD, start : start + size] = tile(ref, span, k).T[HEAD:]
            value_rows[k, HEAD:, start : start + size] = jnp.ones((16, size), BF16)

    work = list(range(low, high, chunk))

    def scores(k, r, slot):
        q = q_ref[pl.ds(k * group, group), r : r + chunk, :].reshape(group * chunk, TILE)
        for ref, span, start, size in zip(blocks, spans, starts, sizes):
            held[slot][start : start + size, :] = lax.dot_general(
                tile(ref, span, k), q, NT, preferred_element_type=F32
            )

    def both(k, value):
        return jnp.concatenate(
            [jnp.full((1, chunk), value[k * group + g], F32) for g in range(group)], axis=1
        )

    def absorb(k, r, slot):
        parts = [(st, held[slot][st : st + n, :]) for st, n in plain]
        if raised:
            extra = both(k, lift)
            parts += [(st, held[slot][st : st + n, :] + extra) for st, n in raised]
        top = functools.reduce(
            jnp.maximum, [jnp.max(x, axis=0, keepdims=True) for _, x in parts]
        )
        if has_state:
            old = [state[k * group + g, :, r : r + chunk] for g in range(group)]
            old = jnp.concatenate(old, axis=1)
            before = old[HEAD + 8 : HEAD + 9]
            top = jnp.maximum(top, before)
        parts.sort(key=lambda part: part[0])
        weights = jnp.concatenate([jnp.exp(x - top).astype(BF16) for _, x in parts], axis=0)
        total = dot(value_rows[k], weights)
        if has_state:
            total = total + old * jnp.exp(before - top)
        if not final:
            for g in range(group):
                lanes = slice(g * chunk, (g + 1) * chunk)
                out = outs[0].at[k * group + g]
                out[0 : HEAD + 8, r : r + chunk] = total[: HEAD + 8, lanes]
                out[HEAD + 8 :, r : r + chunk] = jnp.broadcast_to(top[:, lanes], (8, chunk))
            return
        value = total[:HEAD] / total[HEAD : HEAD + 1]
        whole = [value[:, g * chunk : (g + 1) * chunk] for g in range(group)]
        whole = jnp.concatenate(whole, axis=0).T.astype(BF16)
        size = outs[0].shape[0]
        width = group * HEAD
        for j in range(0, chunk, size):
            outs[(r - low + j) // size][:, pl.ds(aligned(k, width), width)] = whole[j : j + size]

    scores(0, work[0], 0)

    def slot_of(k, i):
        return (k * len(work) + i) % 2 if isinstance(k, int) else i % 2

    def one_head(k):
        for i, r in enumerate(work):
            if i + 1 < len(work):
                scores(k, work[i + 1], slot_of(k, i + 1))
            elif not isinstance(k, int):
                scores(jnp.minimum(k + 1, kv_heads - 1), work[0], slot_of(k, i + 1))
            elif k + 1 < kv_heads:
                scores(k + 1, work[0], slot_of(k, i + 1))
            absorb(k, r, slot_of(k, i))

    if unrolled or len(work) % 2:
        for k in range(kv_heads):
            one_head(k)
    else:
        pl.loop(0, kv_heads)(one_head)


def attention(queries, blocks, lift, state, group, pieces, window=None):
    heads, rows, _ = queries.shape
    kv_heads = heads // group
    low, high = window or (0, rows)
    chunk = min(high - low, 256)
    final = pieces > 0
    spans = [b[1:] for b in blocks]
    keys = sum(end - first for first, _, end in spans)
    lifted = any(end > middle for _, middle, end in spans)
    args = [queries] + [b[0] for b in blocks]
    in_specs = [IN_VMEM] * len(args)
    if lifted:
        in_specs.append(pl.BlockSpec(memory_space=pltpu.SMEM))
        args.append(lift)
    if state is not None:
        in_specs.append(IN_VMEM)
        args.append(state)
    if final:
        out_shape = [jax.ShapeDtypeStruct(((high - low) // pieces, heads * HEAD), BF16)] * pieces
    else:
        out_shape = [jax.ShapeDtypeStruct((heads, STATE, rows), F32)]
    out = pl.pallas_call(
        functools.partial(
            attention_kernel, spans, lifted, state is not None, final, group, chunk, (low, high), True
        ),
        in_specs=in_specs,
        out_specs=[IN_VMEM] * len(out_shape),
        out_shape=out_shape,
        scratch_shapes=[
            pltpu.VMEM((kv_heads, STATE, keys), BF16),
            pltpu.VMEM((keys, group * chunk), F32),
            pltpu.VMEM((keys, group * chunk), F32),
        ],
        compiler_params=pltpu.CompilerParams(vmem_limit_bytes=VMEM_LIMIT),
        cost_estimate=cost(16 * heads * rows * keys * HEAD, 4 * heads * rows * TILE),
        name="attention",
    )(*args)
    return list(out) if final else out[0]


def output_kernel(count, *refs):
    attended = refs[:count]
    weights = refs[count : 2 * count]
    rest, out = refs[2 * count : -1], refs[-1]
    step = min(out.shape[1], 4 * TILE)
    for i in range(0, out.shape[1], step):
        total = None
        for a, w in zip(attended, weights):
            term = dot(a[...], w[:, i : i + step])
            total = term if total is None else total + term
        if rest:
            begun, latent, mod = rest
            gate = [mod[8 * t + 2 : 8 * t + 3, :] for t in range(mod.shape[0] // 8)]
            gate = jnp.concatenate(gate, axis=1)[:, i : i + step]
            total = latent[:, i : i + step].astype(F32) + gate * (begun[:, i : i + step] + total)
        out[:, i : i + step] = total.astype(out.dtype)


def project(attended, weights, begun, latent, mod, depth):
    count = len(attended)
    rows, inner = attended[0].shape
    rest = [] if begun is None else [begun, latent, mod]
    return pl.pallas_call(
        functools.partial(output_kernel, count),
        in_specs=[IN_VMEM] * (2 * count + len(rest)),
        out_specs=IN_VMEM,
        out_shape=jax.ShapeDtypeStruct((rows, depth), BF16 if rest else F32),
        compiler_params=pltpu.CompilerParams(vmem_limit_bytes=VMEM_LIMIT),
        cost_estimate=cost(2 * rows * depth * inner * count, 2 * depth * inner * count),
        name="output",
    )(*attended, *weights, *rest)


def rotary_tables(rank, tp, rows, context_rows):
    index = lax.broadcasted_iota(jnp.int32, (tp * rows + context_rows, TILE), 0)
    lane = lax.broadcasted_iota(jnp.int32, (tp * rows + context_rows, TILE), 1)
    piece = index // rows
    position = (rank // tp * tp + jnp.bitwise_xor(rank % tp, piece)) * rows + index % rows
    quarter = HEAD // 4
    pair = lane % HEAD // 2
    frequency = ROTARY_BASE ** (-(pair % quarter).astype(F32) / quarter)
    place = jnp.where(pair < quarter, position // GRID, position % GRID).astype(F32)
    angle = jnp.where(index < tp * rows, place, 0.0) * frequency
    sine = jnp.sin(angle)
    even = lane % 2 == 0
    return jnp.cos(angle), jnp.where(even, -sine, 0.0), jnp.where(even, 0.0, sine)


def shards(
    sp,
    tp,
    latent,
    context,
    conditioning,
    context_conditioning,
    shift_weight,
    scale_weight,
    gate_weight,
    norm_gain,
    query_weight,
    key_weight,
    value_weight,
    query_gain,
    key_gain,
    context_lift,
    output_weight,
):
    rows = latent.shape[0]
    length = rows * tp
    context_rows = context.shape[0]
    group = query_weight.shape[1] // key_weight.shape[1]
    tp_bits = [1 << b for b in reversed(range(tp.bit_length() - 1))]

    def spread(have, bit):
        have.update({j | bit: swap(v, "tp", tp, bit) for j, v in list(have.items())})

    def tie(*values):
        return lax.optimization_barrier(values)

    pieces = {0: latent}
    spread(pieces, tp_bits[0])
    partial = modulation_partial(
        conditioning, context_conditioning, shift_weight, scale_weight, gate_weight
    )
    rank = lax.axis_index("sp") * tp + lax.axis_index("tp")
    gains = [v.reshape(1, -1) for v in (norm_gain, key_gain, query_gain)]
    early = [
        (*rotary_tables(rank, tp, rows, context_rows), jnp.concatenate(gains, axis=1)),
        (jnp.concatenate([key_weight, value_weight], axis=1),),
    ]
    ready = []
    bits = [1 << b for b in range(sp.bit_length() - 1)]
    for i in range(0, len(bits), 2):
        pair = bits[i : i + 2]
        masks = pair + [sum(pair)] if len(pair) == 2 else pair
        arrived = [swap(partial, "sp", sp, m) for m in masks]
        extra = early.pop(0) if early else ()
        tied = tie(*arrived, *extra)
        partial = sum(tied[: len(arrived)], partial)
        ready += tied[len(arrived) :]
    for extra in early:
        ready += extra
    *tables, gains, kv_weight = ready
    partial, pieces[tp_bits[0]] = tie(partial, pieces[tp_bits[0]])
    for bit in tp_bits[1:]:
        spread(pieces, bit)
    mod = lax.all_gather(partial, "tp", axis=0, tiled=True)

    hidden, first, second = keys_values(
        [pieces[j] for j in range(tp)], context, mod, gains, kv_weight, tables
    )

    half = length // 2
    order = list(range(0, sp, 2)) + list(range(sp - 1, 0, -2))
    ahead = [(order[i], order[(i + 1) % sp]) for i in range(sp)]
    back = [(b, a) for a, b in ahead]

    def hop(pair):
        return lax.ppermute(pair[0], "sp", ahead), lax.ppermute(pair[1], "sp", back)

    def as_blocks(pair):
        return [(b, 0, half, half if b.shape[0] == half else half + context_rows) for b in pair]

    flight = [hop((first, second))]
    flight.append(hop((second, first)))
    queries = queries_of(hidden, query_weight, gains, tables, length)
    output_weight, _ = tie(output_weight, first)
    weights = {0: output_weight}
    spread(weights, tp_bits[0])
    waiting = as_blocks((first, second))
    state = None
    for i in range(sp - 1):
        state = attention(queries, waiting, context_lift, state, group, 0)
        up, down, state = tie(*flight.pop(0), state)
        if i < sp - 3:
            flight.append(hop((up, down)))
        waiting = as_blocks((up, down))
    far = attention(queries, waiting, context_lift, state, group, tp // 2, (half, length))
    top_bit = tp_bits[0]
    weights[top_bit], state, *_ = tie(weights[top_bit], state, *far)
    for bit in tp_bits[1:]:
        spread(weights, bit)
    far = [swap(a, "tp", tp, tp // 2 + j) for j, a in enumerate(far)]
    near = attention(queries, waiting, context_lift, state, group, tp // 2, (0, half))
    near = near[:1] + [swap(a, "tp", tp, j) for j, a in enumerate(near) if j]
    weights = [weights[j] for j in range(tp)]
    begun = project(near, weights[: tp // 2], None, None, None, latent.shape[1])
    return project(far, weights[tp // 2 :], begun, latent, mod, latent.shape[1])


def solution(mesh):
    in_specs = (
        P(("sp", "tp"), None),
        P("sp", None),
        P("sp"),
        P("sp"),
        P("sp", "tp"),
        P("sp", "tp"),
        P("sp", "tp"),
        P(),
        P(None, "tp"),
        P(None, "tp"),
        P(None, "tp"),
        P(),
        P(),
        P("tp"),
        P("tp", None),
    )
    return jax.shard_map(
        functools.partial(shards, mesh.shape["sp"], mesh.shape["tp"]),
        mesh=mesh,
        in_specs=in_specs,
        out_specs=P(("sp", "tp"), None),
        check_vma=False,
    )
```

```python
import functools

import jax
import jax.numpy as jnp
from jax import lax
from jax.experimental import pallas as pl
from jax.experimental.pallas import tpu as pltpu
from jax.sharding import PartitionSpec as P


HEAD = 64
GRID = 64
TILE = 128
EPSILON = 1e-06
ROTARY_BASE = 10000.0
F32 = jnp.float32
BF16 = jnp.bfloat16


VMEM_LIMIT = 20 << 20
IN_VMEM = pl.BlockSpec(memory_space=pltpu.VMEM)

NT = (((1,), (1,)), ((), ()))


def dot(a, b):
    return jnp.dot(a, b, preferred_element_type=F32)


def cost(flops, nbytes):
    return pl.CostEstimate(flops=int(flops), bytes_accessed=int(nbytes), transcendentals=0)


def swap(value, axis, size, mask):
    return lax.ppermute(value, axis, [(i, i ^ mask) for i in range(size)])


def modulation_kernel(cond, ccond, shift, scale, gate, out):
    def signal(ref):
        v = ref[...]
        return (v / (1.0 + jnp.exp(-v))).astype(BF16)

    both = jnp.concatenate([signal(cond), signal(ccond)], axis=0)
    both = jnp.concatenate([both, jnp.zeros((6,) + both.shape[1:], F32).astype(BF16)], axis=0)
    s = dot(both, shift[...])
    c = dot(both, scale[...])
    g = dot(both, gate[...])
    out[0:1, :] = s[0:1]
    out[1:2, :] = c[0:1]
    out[2:3, :] = g[0:1]
    out[3:4, :] = s[1:2]
    out[4:5, :] = c[1:2]
    out[5:8, :] = jnp.zeros((3, out.shape[1]), F32)


def modulation_partial(cond, ccond, shift, scale, gate):
    width = shift.shape[1]
    depth = cond.shape[0]
    return pl.pallas_call(
        modulation_kernel,
        out_shape=jax.ShapeDtypeStruct((8, width), F32),
        cost_estimate=cost(6 * 8 * depth * width, 6 * depth * width),
        name="modulation",
    )(cond.reshape(1, depth), ccond.reshape(1, depth), shift, scale, gate)


def head_scale(x):
    width = x.shape[1]
    square = x * x
    high = square.astype(BF16)
    low = (square - high.astype(F32)).astype(BF16)
    rows = lax.broadcasted_iota(jnp.int32, (width, width), 0) // HEAD
    cols = lax.broadcasted_iota(jnp.int32, (width, width), 1) // HEAD
    ones = jnp.where(rows == cols, 1.0, 0.0).astype(BF16)
    mean = (dot(high, ones) + dot(low, ones)) * (1.0 / HEAD)
    return lax.rsqrt(mean + EPSILON)


def turn(x, tables):
    width = x.shape[1]
    left = pltpu.roll(x, width - 1, 1)
    right = pltpu.roll(x, 1, 1)
    return x * tables[0] + left * tables[1] + right * tables[2]


def pieces_of(x, width):
    return [x[:, i : i + width] for i in range(0, x.shape[1], width)]


def finish_heads(x, gain, tables):
    out = []
    step = TILE if x.shape[1] % TILE == 0 else HEAD
    tables = [t[:, :step] for t in tables]
    gain = jnp.concatenate([gain] * (step // HEAD), axis=1)
    for part in pieces_of(x, step):
        out.append(turn(part * head_scale(part) * gain, tables))
    return [h for part in out for h in pieces_of(part, HEAD)]


def modulate(x, gain, shift, dest, row):
    rows = x.shape[0]
    x = x.astype(F32)
    inverse = lax.rsqrt(jnp.mean(x * x, axis=1, keepdims=True) + EPSILON)
    dest[row : row + rows, :] = (x * inverse * gain + shift).astype(BF16)


def kv_kernel(count, *refs):
    pieces = refs[:count]
    context, mod, gains, weight, cos, sin_e, sin_o = refs[count : count + 7]
    hidden, first, second = refs[count + 7 :]
    extra = context.shape[0] // 2
    half = first.shape[0] - extra
    norm_gain = gains[:, : context.shape[1]]
    key_gain = gains[:, context.shape[1] : context.shape[1] + HEAD]
    parts = mod.shape[0] // 8

    def vector(index):
        return jnp.concatenate([mod[8 * t + index : 8 * t + index + 1, :] for t in range(parts)], axis=1)

    gain = norm_gain * (1.0 + vector(1))
    shift = vector(0)
    row = 0
    for piece in pieces:
        modulate(piece[...], gain, shift, hidden, row)
        row += piece.shape[0]
    modulate(context[...], norm_gain * (1.0 + vector(4)), vector(3), hidden, row)
    h = hidden[...]
    width = weight.shape[1] // 2
    keys = dot(h, weight[:, :width])
    values = dot(h, weight[:, width:])
    tables = (cos[...], sin_e[...], sin_o[...])
    heads = finish_heads(keys, key_gain, tables)
    for k, key in enumerate(heads):
        tile = jnp.concatenate([key, values[:, k * HEAD : (k + 1) * HEAD]], axis=1).astype(BF16)
        lanes = slice(k * TILE, (k + 1) * TILE)
        first[:half, lanes] = tile[:half]
        first[half:, lanes] = tile[2 * half : 2 * half + extra]
        second[:half, lanes] = tile[half : 2 * half]
        second[half:, lanes] = tile[2 * half + extra :]


def keys_values(pieces, context, mod, gains, weight, tables):
    rows = sum(p.shape[0] for p in pieces) + context.shape[0]
    depth = context.shape[1]
    width = weight.shape[1] // 2
    return pl.pallas_call(
        functools.partial(kv_kernel, len(pieces)),
        out_shape=(
            jax.ShapeDtypeStruct((rows, depth), BF16),
            jax.ShapeDtypeStruct((rows // 2, 2 * width), BF16),
            jax.ShapeDtypeStruct((rows // 2, 2 * width), BF16),
        ),
        in_specs=[IN_VMEM] * (len(pieces) + 7),
        out_specs=(IN_VMEM, IN_VMEM, IN_VMEM),
        compiler_params=pltpu.CompilerParams(vmem_limit_bytes=VMEM_LIMIT),
        cost_estimate=cost(4 * rows * depth * width, 4 * rows * depth + 4 * depth * width),
        name="keys_values",
    )(*pieces, context, mod, gains, weight, *tables)


def query_kernel(hidden, weight, gains, cos, sin_e, sin_o, out):
    rows = out.shape[1]
    tables = (cos[0:rows, :], sin_e[0:rows, :], sin_o[0:rows, :])
    gain = gains[:, hidden.shape[1] + HEAD :]
    x = dot(hidden[0:rows, :], weight[...])
    for i, head in enumerate(finish_heads(x, gain, tables)):
        head = (head * (HEAD**-0.5)).astype(BF16)
        out[i] = jnp.concatenate([head, jnp.zeros_like(head)], axis=1)


def queries_of(hidden, weight, gains, tables, rows):
    depth, width = weight.shape
    return pl.pallas_call(
        query_kernel,
        in_specs=[IN_VMEM] * 6,
        out_specs=IN_VMEM,
        out_shape=jax.ShapeDtypeStruct((width // HEAD, rows, TILE), BF16),
        compiler_params=pltpu.CompilerParams(vmem_limit_bytes=VMEM_LIMIT),
        cost_estimate=cost(2 * rows * depth * width, 2 * rows * depth + 2 * depth * width),
        name="queries",
    )(hidden, weight, gains, *tables)


STATE = HEAD + 16


def attention_kernel(spans, lifted, has_state, final, group, chunk, window, unrolled, *refs):
    refs = list(refs)
    q_ref = refs.pop(0)
    blocks = [refs.pop(0) for _ in spans]
    lift = refs.pop(0) if lifted else None
    state = refs.pop(0) if has_state else None
    value_rows, held = refs[-3], refs[-2:]
    outs = refs[:-3]
    low, high = window
    kv_heads = q_ref.shape[0] // group
    sizes = [end - first for first, _, end in spans]
    starts = [sum(sizes[:i]) for i in range(len(sizes))]
    plain = [(st, middle - first) for st, (first, middle, _) in zip(starts, spans) if middle > first]
    raised = [
        (st + middle - first, end - middle)
        for st, (first, middle, end) in zip(starts, spans)
        if end > middle
    ]

    def aligned(k, width):
        return k * width if isinstance(k, int) else pl.multiple_of(k * width, width)

    def tile(ref, span, k):
        return ref[span[0] : span[2], pl.ds(aligned(k, TILE), TILE)]

    for k in range(kv_heads):
        for ref, span, start, size in zip(blocks, spans, starts, sizes):
            value_rows[k, 0:HEAD, start : start + size] = tile(ref, span, k).T[HEAD:]
            value_rows[k, HEAD:, start : start + size] = jnp.ones((16, size), BF16)

    work = list(range(low, high, chunk))

    def scores(k, r, slot):
        q = q_ref[pl.ds(k * group, group), r : r + chunk, :].reshape(group * chunk, TILE)
        for ref, span, start, size in zip(blocks, spans, starts, sizes):
            held[slot][start : start + size, :] = lax.dot_general(
                tile(ref, span, k), q, NT, preferred_element_type=F32
            )

    def raises(k):
        heads = [lift[k * group + g, 0:1, :] for g in range(group)]
        return jnp.concatenate([h for h in heads for _ in range(chunk // TILE)], axis=1)

    def absorb(k, r, slot):
        parts = [(st, held[slot][st : st + n, :]) for st, n in plain]
        if raised:
            extra = raises(k)
            parts += [(st, held[slot][st : st + n, :] + extra) for st, n in raised]
        top = functools.reduce(
            jnp.maximum, [jnp.max(x, axis=0, keepdims=True) for _, x in parts]
        )
        if has_state:
            old = [state[k * group + g, :, r : r + chunk] for g in range(group)]
            old = jnp.concatenate(old, axis=1)
            before = old[HEAD + 8 : HEAD + 9]
            top = jnp.maximum(top, before)
        parts.sort(key=lambda part: part[0])
        weights = jnp.concatenate([jnp.exp(x - top).astype(BF16) for _, x in parts], axis=0)
        total = dot(value_rows[k], weights)
        if has_state:
            total = total + old * jnp.exp(before - top)
        if not final:
            for g in range(group):
                lanes = slice(g * chunk, (g + 1) * chunk)
                out = outs[0].at[k * group + g]
                out[0 : HEAD + 8, r : r + chunk] = total[: HEAD + 8, lanes]
                out[HEAD + 8 :, r : r + chunk] = jnp.broadcast_to(top[:, lanes], (8, chunk))
            return
        value = total[:HEAD] / total[HEAD : HEAD + 1]
        whole = [value[:, g * chunk : (g + 1) * chunk] for g in range(group)]
        whole = jnp.concatenate(whole, axis=0).T.astype(BF16)
        size = outs[0].shape[0]
        width = group * HEAD
        for j in range(0, chunk, size):
            outs[(r - low + j) // size][:, pl.ds(aligned(k, width), width)] = whole[j : j + size]

    scores(0, work[0], 0)

    def slot_of(k, i):
        return (k * len(work) + i) % 2 if isinstance(k, int) else i % 2

    def one_head(k):
        for i, r in enumerate(work):
            if i + 1 < len(work):
                scores(k, work[i + 1], slot_of(k, i + 1))
            elif not isinstance(k, int):
                scores(jnp.minimum(k + 1, kv_heads - 1), work[0], slot_of(k, i + 1))
            elif k + 1 < kv_heads:
                scores(k + 1, work[0], slot_of(k, i + 1))
            absorb(k, r, slot_of(k, i))

    if unrolled or len(work) % 2:
        for k in range(kv_heads):
            one_head(k)
    else:
        pl.loop(0, kv_heads)(one_head)


def attention(queries, blocks, lift, state, group, pieces, window=None):
    heads, rows, _ = queries.shape
    kv_heads = heads // group
    low, high = window or (0, rows)
    chunk = min(high - low, 256)
    final = pieces > 0
    spans = [b[1:] for b in blocks]
    keys = sum(end - first for first, _, end in spans)
    lifted = any(end > middle for _, middle, end in spans)
    args = [queries] + [b[0] for b in blocks]
    in_specs = [IN_VMEM] * len(args)
    if lifted:
        in_specs.append(IN_VMEM)
        args.append(lift)
    if state is not None:
        in_specs.append(IN_VMEM)
        args.append(state)
    if final:
        out_shape = [jax.ShapeDtypeStruct(((high - low) // pieces, heads * HEAD), BF16)] * pieces
    else:
        out_shape = [jax.ShapeDtypeStruct((heads, STATE, rows), F32)]
    out = pl.pallas_call(
        functools.partial(
            attention_kernel, spans, lifted, state is not None, final, group, chunk, (low, high), True
        ),
        in_specs=in_specs,
        out_specs=[IN_VMEM] * len(out_shape),
        out_shape=out_shape,
        scratch_shapes=[
            pltpu.VMEM((kv_heads, STATE, keys), BF16),
            pltpu.VMEM((keys, group * chunk), F32),
            pltpu.VMEM((keys, group * chunk), F32),
        ],
        compiler_params=pltpu.CompilerParams(vmem_limit_bytes=VMEM_LIMIT),
        cost_estimate=cost(16 * heads * rows * keys * HEAD, 4 * heads * rows * TILE),
        name="attention",
    )(*args)
    return list(out) if final else out[0]


def output_kernel(count, *refs):
    attended = refs[:count]
    weights = refs[count : 2 * count]
    rest = refs[2 * count : -3] if len(refs) > 2 * count + 1 else ()
    out = refs[-3] if rest else refs[-1]
    step = min(out.shape[1], 4 * TILE)
    copies = []
    for i in range(0, out.shape[1], step):
        total = None
        for a, w in zip(attended, weights):
            term = dot(a[...], w[:, i : i + step])
            total = term if total is None else total + term
        if rest:
            begun, latent, mod = rest
            gate = [mod[8 * t + 2 : 8 * t + 3, :] for t in range(mod.shape[0] // 8)]
            gate = jnp.concatenate(gate, axis=1)[:, i : i + step]
            total = latent[:, i : i + step].astype(F32) + gate * (begun[:, i : i + step] + total)
            made, sems = refs[-2:]
            made[:, i : i + step] = total.astype(out.dtype)
            lanes = pl.ds(i, step)
            copy = pltpu.make_async_copy(made.at[:, lanes], out.at[:, lanes], sems.at[i // step])
            copy.start()
            copies.append(copy)
        else:
            out[:, i : i + step] = total
    for copy in copies:
        copy.wait()


def project(attended, weights, begun, latent, mod, depth):
    count = len(attended)
    rows, inner = attended[0].shape
    rest = [] if begun is None else [begun, latent, mod]
    return pl.pallas_call(
        functools.partial(output_kernel, count),
        in_specs=[IN_VMEM] * (2 * count + len(rest)),
        out_specs=pl.BlockSpec(memory_space=pltpu.HBM) if rest else IN_VMEM,
        out_shape=jax.ShapeDtypeStruct((rows, depth), BF16 if rest else F32),
        scratch_shapes=[
            pltpu.VMEM((rows, depth), BF16),
            pltpu.SemaphoreType.DMA((pl.cdiv(depth, 4 * TILE),)),
        ]
        if rest
        else [],
        compiler_params=pltpu.CompilerParams(vmem_limit_bytes=VMEM_LIMIT),
        cost_estimate=cost(2 * rows * depth * inner * count, 2 * depth * inner * count),
        name="output",
    )(*attended, *weights, *rest)


def rotary_tables(rank, tp, rows, context_rows):
    index = lax.broadcasted_iota(jnp.int32, (tp * rows + context_rows, TILE), 0)
    lane = lax.broadcasted_iota(jnp.int32, (tp * rows + context_rows, TILE), 1)
    piece = index // rows
    position = (rank // tp * tp + jnp.bitwise_xor(rank % tp, piece)) * rows + index % rows
    quarter = HEAD // 4
    pair = lane % HEAD // 2
    frequency = ROTARY_BASE ** (-(pair % quarter).astype(F32) / quarter)
    place = jnp.where(pair < quarter, position // GRID, position % GRID).astype(F32)
    angle = jnp.where(index < tp * rows, place, 0.0) * frequency
    sine = jnp.sin(angle)
    even = lane % 2 == 0
    return jnp.cos(angle), jnp.where(even, -sine, 0.0), jnp.where(even, 0.0, sine)


def shards(
    sp,
    tp,
    latent,
    context,
    conditioning,
    context_conditioning,
    shift_weight,
    scale_weight,
    gate_weight,
    norm_gain,
    query_weight,
    key_weight,
    value_weight,
    query_gain,
    key_gain,
    context_lift,
    output_weight,
):
    rows = latent.shape[0]
    length = rows * tp
    context_rows = context.shape[0]
    group = query_weight.shape[1] // key_weight.shape[1]
    tp_bits = [1 << b for b in reversed(range(tp.bit_length() - 1))]

    def spread(have, bit):
        have.update({j | bit: swap(v, "tp", tp, bit) for j, v in list(have.items())})

    def tie(*values):
        return lax.optimization_barrier(values)

    pieces = {0: latent}
    spread(pieces, tp_bits[0])
    partial = modulation_partial(
        conditioning, context_conditioning, shift_weight, scale_weight, gate_weight
    )
    rank = lax.axis_index("sp") * tp + lax.axis_index("tp")
    gains = [v.reshape(1, -1) for v in (norm_gain, key_gain, query_gain)]
    early = [
        (*rotary_tables(rank, tp, rows, context_rows), jnp.concatenate(gains, axis=1)),
        (
            jnp.concatenate([key_weight, value_weight], axis=1),
            jnp.broadcast_to(context_lift[:, None, None], context_lift.shape + (8, TILE)),
        ),
    ]
    ready = []
    bits = [1 << b for b in range(sp.bit_length() - 1)]
    for i in range(0, len(bits), 2):
        pair = bits[i : i + 2]
        masks = pair + [sum(pair)] if len(pair) == 2 else pair
        arrived = []
        for m in masks:
            arrived.append(swap(partial, "sp", sp, m))
        extra = early.pop(0) if early else ()
        tied = tie(*arrived, *extra)
        partial = sum(tied[: len(arrived)], partial)
        ready += tied[len(arrived) :]
    for extra in early:
        ready += extra
    *tables, gains, kv_weight, lifts = ready
    partial, pieces[tp_bits[0]] = tie(partial, pieces[tp_bits[0]])
    for bit in tp_bits[1:]:
        spread(pieces, bit)
    mod = lax.all_gather(partial, "tp", axis=0, tiled=True)

    hidden, first, second = keys_values(
        [pieces[j] for j in range(tp)], context, mod, gains, kv_weight, tables
    )

    half = length // 2
    order = list(range(0, sp, 2)) + list(range(sp - 1, 0, -2))
    ahead = [(order[i], order[(i + 1) % sp]) for i in range(sp)]
    back = [(b, a) for a, b in ahead]

    def hop(pair):
        return lax.ppermute(pair[0], "sp", ahead), lax.ppermute(pair[1], "sp", back)

    def as_blocks(pair):
        return [(b, 0, half, b.shape[0]) for b in pair]

    flight = [hop((first, second))]
    flight.append(hop((second, first)))
    queries = queries_of(hidden, query_weight, gains, tables, length)
    output_weight, _ = tie(output_weight, first)
    weights = {0: output_weight}
    spread(weights, tp_bits[0])
    waiting = as_blocks((first, second))
    state = None
    for i in range(sp - 1):
        state = attention(queries, waiting, lifts, state, group, 0)
        up, down, state = tie(*flight.pop(0), state)
        if i < sp - 3:
            flight.append(hop((up, down)))
        waiting = as_blocks((up, down))
    far = attention(queries, waiting, lifts, state, group, tp // 2, (half, length))
    top_bit = tp_bits[0]
    weights[top_bit], state, *_ = tie(weights[top_bit], state, *far)
    for bit in tp_bits[1:]:
        spread(weights, bit)
    far = [swap(a, "tp", tp, tp // 2 + j) for j, a in enumerate(far)]
    near = attention(queries, waiting, lifts, state, group, tp // 2, (0, half))
    near = near[:1] + [swap(a, "tp", tp, j) for j, a in enumerate(near) if j]
    weights = [weights[j] for j in range(tp)]
    begun = project(near, weights[: tp // 2], None, None, None, latent.shape[1])
    return project(far, weights[tp // 2 :], begun, latent, mod, latent.shape[1])


def solution(mesh):
    in_specs = (
        P(("sp", "tp"), None),
        P("sp", None),
        P("sp"),
        P("sp"),
        P("sp", "tp"),
        P("sp", "tp"),
        P("sp", "tp"),
        P(),
        P(None, "tp"),
        P(None, "tp"),
        P(None, "tp"),
        P(),
        P(),
        P("tp"),
        P("tp", None),
    )
    return jax.shard_map(
        functools.partial(shards, mesh.shape["sp"], mesh.shape["tp"]),
        mesh=mesh,
        in_specs=in_specs,
        out_specs=P(("sp", "tp"), None),
        check_vma=False,
    )
```

```python
import functools

import jax
import jax.numpy as jnp
from jax import lax
from jax.experimental import pallas as pl
from jax.experimental.pallas import tpu as pltpu
from jax.sharding import PartitionSpec as P


HEAD = 64
GRID = 64
TILE = 128
EPSILON = 1e-06
ROTARY_BASE = 10000.0
F32 = jnp.float32
BF16 = jnp.bfloat16


VMEM_LIMIT = 20 << 20
IN_VMEM = pl.BlockSpec(memory_space=pltpu.VMEM)

NT = (((1,), (1,)), ((), ()))


def dot(a, b):
    return jnp.dot(a, b, preferred_element_type=F32)


def cost(flops, nbytes):
    return pl.CostEstimate(flops=int(flops), bytes_accessed=int(nbytes), transcendentals=0)


def swap(value, axis, size, mask):
    return lax.ppermute(value, axis, [(i, i ^ mask) for i in range(size)])


def modulation_kernel(cond, ccond, shift, scale, gate, out):
    def signal(ref):
        v = ref[...]
        return (v / (1.0 + jnp.exp(-v))).astype(BF16)

    both = jnp.concatenate([signal(cond), signal(ccond)], axis=0)
    both = jnp.concatenate([both, jnp.zeros((6,) + both.shape[1:], F32).astype(BF16)], axis=0)
    s = dot(both, shift[...])
    c = dot(both, scale[...])
    g = dot(both, gate[...])
    out[0:1, :] = s[0:1]
    out[1:2, :] = c[0:1]
    out[2:3, :] = g[0:1]
    out[3:4, :] = s[1:2]
    out[4:5, :] = c[1:2]
    out[5:8, :] = jnp.zeros((3, out.shape[1]), F32)


def modulation_partial(cond, ccond, shift, scale, gate):
    width = shift.shape[1]
    depth = cond.shape[0]
    return pl.pallas_call(
        modulation_kernel,
        out_shape=jax.ShapeDtypeStruct((8, width), F32),
        cost_estimate=cost(6 * 8 * depth * width, 6 * depth * width),
        name="modulation",
    )(cond.reshape(1, depth), ccond.reshape(1, depth), shift, scale, gate)


def head_scale(x):
    width = x.shape[1]
    square = x * x
    high = square.astype(BF16)
    low = (square - high.astype(F32)).astype(BF16)
    rows = lax.broadcasted_iota(jnp.int32, (width, width), 0) // HEAD
    cols = lax.broadcasted_iota(jnp.int32, (width, width), 1) // HEAD
    ones = jnp.where(rows == cols, 1.0, 0.0).astype(BF16)
    mean = (dot(high, ones) + dot(low, ones)) * (1.0 / HEAD)
    return lax.rsqrt(mean + EPSILON)


def turn(x, tables):
    width = x.shape[1]
    left = pltpu.roll(x, width - 1, 1)
    right = pltpu.roll(x, 1, 1)
    return x * tables[0] + left * tables[1] + right * tables[2]


def pieces_of(x, width):
    return [x[:, i : i + width] for i in range(0, x.shape[1], width)]


def finish_heads(x, gain, tables):
    out = []
    step = TILE if x.shape[1] % TILE == 0 else HEAD
    tables = [t[:, :step] for t in tables]
    gain = jnp.concatenate([gain] * (step // HEAD), axis=1)
    for part in pieces_of(x, step):
        out.append(turn(part * head_scale(part) * gain, tables))
    return [h for part in out for h in pieces_of(part, HEAD)]


def normal_kernel(*refs):
    out = refs[-1]
    row = 0
    for ref in refs[:-1]:
        x = ref[...].astype(F32)
        inverse = lax.rsqrt(jnp.mean(x * x, axis=1, keepdims=True) + EPSILON)
        out[row : row + x.shape[0], :] = x * inverse
        row += x.shape[0]


def normal_rows(arrays):
    rows = sum(x.shape[0] for x in arrays)
    depth = arrays[0].shape[1]
    return pl.pallas_call(
        normal_kernel,
        in_specs=[IN_VMEM] * len(arrays),
        out_specs=IN_VMEM,
        out_shape=jax.ShapeDtypeStruct((rows, depth), F32),
        compiler_params=pltpu.CompilerParams(vmem_limit_bytes=VMEM_LIMIT),
        cost_estimate=cost(8 * rows * depth, 6 * rows * depth),
        name="normal",
    )(*arrays)


def kv_kernel(count, context_rows, *refs):
    tails = refs[:count]
    normal, gains, weight, cos, sin_e, sin_o = refs[count : count + 6]
    hidden, first, second, mod = refs[count + 6 :]
    extra = context_rows // 2
    half = first.shape[0] - extra
    norm_gain = gains[:, : normal.shape[1]]
    key_gain = gains[:, normal.shape[1] : normal.shape[1] + HEAD]
    rank = lax.axis_index("tp")
    for j, tail in enumerate(tails):
        mod[jnp.bitwise_xor(rank, j)] = tail[...]

    def vector(index):
        return jnp.concatenate([mod[t, index : index + 1, :] for t in range(count)], axis=1)

    length = 2 * half
    gain, context_gain = [norm_gain * (1.0 + vector(i)) for i in (1, 4)]
    hidden[:length, :] = (normal[:length, :] * gain + vector(0)).astype(BF16)
    hidden[length:, :] = (normal[length:, :] * context_gain + vector(3)).astype(BF16)
    h = hidden[...]
    width = weight.shape[1] // 2
    keys = dot(h, weight[:, :width])
    values = dot(h, weight[:, width:])
    tables = (cos[...], sin_e[...], sin_o[...])
    heads = finish_heads(keys, key_gain, tables)
    for k, key in enumerate(heads):
        tile = jnp.concatenate([key, values[:, k * HEAD : (k + 1) * HEAD]], axis=1).astype(BF16)
        lanes = slice(k * TILE, (k + 1) * TILE)
        first[:half, lanes] = tile[:half]
        first[half:, lanes] = tile[2 * half : 2 * half + extra]
        second[:half, lanes] = tile[half : 2 * half]
        second[half:, lanes] = tile[2 * half + extra :]


def keys_values(normal, context_rows, tails, gains, weight, tables):
    rows, depth = normal.shape
    width = weight.shape[1] // 2
    return pl.pallas_call(
        functools.partial(kv_kernel, len(tails), context_rows),
        out_shape=(
            jax.ShapeDtypeStruct((rows, depth), BF16),
            jax.ShapeDtypeStruct((rows // 2, 2 * width), BF16),
            jax.ShapeDtypeStruct((rows // 2, 2 * width), BF16),
            jax.ShapeDtypeStruct((len(tails),) + tails[0].shape, F32),
        ),
        in_specs=[IN_VMEM] * (len(tails) + 6),
        out_specs=(IN_VMEM,) * 4,
        compiler_params=pltpu.CompilerParams(vmem_limit_bytes=VMEM_LIMIT),
        cost_estimate=cost(4 * rows * depth * width, 4 * rows * depth + 4 * depth * width),
        name="keys_values",
    )(*tails, normal, gains, weight, *tables)


def query_kernel(hidden, weight, gains, cos, sin_e, sin_o, out):
    rows = out.shape[1]
    tables = (cos[0:rows, :], sin_e[0:rows, :], sin_o[0:rows, :])
    gain = gains[:, hidden.shape[1] + HEAD :]
    x = dot(hidden[0:rows, :], weight[...])
    for i, head in enumerate(finish_heads(x, gain, tables)):
        head = (head * (HEAD**-0.5)).astype(BF16)
        out[i] = jnp.concatenate([head, jnp.zeros_like(head)], axis=1)


def queries_of(hidden, weight, gains, tables, rows):
    depth, width = weight.shape
    return pl.pallas_call(
        query_kernel,
        in_specs=[IN_VMEM] * 6,
        out_specs=IN_VMEM,
        out_shape=jax.ShapeDtypeStruct((width // HEAD, rows, TILE), BF16),
        compiler_params=pltpu.CompilerParams(vmem_limit_bytes=VMEM_LIMIT),
        cost_estimate=cost(2 * rows * depth * width, 2 * rows * depth + 2 * depth * width),
        name="queries",
    )(hidden, weight, gains, *tables)


STATE = HEAD + 16


def attention_kernel(spans, lifted, has_state, final, group, chunk, window, unrolled, *refs):
    refs = list(refs)
    q_ref = refs.pop(0)
    blocks = [refs.pop(0) for _ in spans]
    lift = refs.pop(0) if lifted else None
    state = refs.pop(0) if has_state else None
    value_rows, held = refs[-3], refs[-2:]
    outs = refs[:-3]
    low, high = window
    kv_heads = q_ref.shape[0] // group
    sizes = [end - first for first, _, end in spans]
    starts = [sum(sizes[:i]) for i in range(len(sizes))]
    plain = [(st, middle - first) for st, (first, middle, _) in zip(starts, spans) if middle > first]
    raised = [
        (st + middle - first, end - middle)
        for st, (first, middle, end) in zip(starts, spans)
        if end > middle
    ]

    def aligned(k, width):
        return k * width if isinstance(k, int) else pl.multiple_of(k * width, width)

    def tile(ref, span, k):
        return ref[span[0] : span[2], pl.ds(aligned(k, TILE), TILE)]

    for k in range(kv_heads):
        for ref, span, start, size in zip(blocks, spans, starts, sizes):
            value_rows[k, 0:HEAD, start : start + size] = tile(ref, span, k).T[HEAD:]
            value_rows[k, HEAD:, start : start + size] = jnp.ones((16, size), BF16)

    work = list(range(low, high, chunk))

    def scores(k, r, slot):
        q = q_ref[pl.ds(k * group, group), r : r + chunk, :].reshape(group * chunk, TILE)
        for ref, span, start, size in zip(blocks, spans, starts, sizes):
            held[slot][start : start + size, :] = lax.dot_general(
                tile(ref, span, k), q, NT, preferred_element_type=F32
            )

    def raises(k):
        heads = [lift[k * group + g, 0:1, :] for g in range(group)]
        return jnp.concatenate([h for h in heads for _ in range(chunk // TILE)], axis=1)

    def absorb(k, r, slot):
        parts = [(st, held[slot][st : st + n, :]) for st, n in plain]
        if raised:
            extra = raises(k)
            parts += [(st, held[slot][st : st + n, :] + extra) for st, n in raised]
        top = functools.reduce(
            jnp.maximum, [jnp.max(x, axis=0, keepdims=True) for _, x in parts]
        )
        if has_state:
            old = [state[k * group + g, :, r : r + chunk] for g in range(group)]
            old = jnp.concatenate(old, axis=1)
            before = old[HEAD + 8 : HEAD + 9]
            top = jnp.maximum(top, before)
        parts.sort(key=lambda part: part[0])
        weights = jnp.concatenate([jnp.exp(x - top).astype(BF16) for _, x in parts], axis=0)
        total = dot(value_rows[k], weights)
        if has_state:
            total = total + old * jnp.exp(before - top)
        if not final:
            for g in range(group):
                lanes = slice(g * chunk, (g + 1) * chunk)
                out = outs[0].at[k * group + g]
                out[0 : HEAD + 8, r : r + chunk] = total[: HEAD + 8, lanes]
                out[HEAD + 8 :, r : r + chunk] = jnp.broadcast_to(top[:, lanes], (8, chunk))
            return
        value = total[:HEAD] / total[HEAD : HEAD + 1]
        whole = [value[:, g * chunk : (g + 1) * chunk] for g in range(group)]
        whole = jnp.concatenate(whole, axis=0).T.astype(BF16)
        size = outs[0].shape[0]
        width = group * HEAD
        for j in range(0, chunk, size):
            outs[(r - low + j) // size][:, pl.ds(aligned(k, width), width)] = whole[j : j + size]

    scores(0, work[0], 0)

    def slot_of(k, i):
        return (k * len(work) + i) % 2 if isinstance(k, int) else i % 2

    def one_head(k):
        for i, r in enumerate(work):
            if i + 1 < len(work):
                scores(k, work[i + 1], slot_of(k, i + 1))
            elif not isinstance(k, int):
                scores(jnp.minimum(k + 1, kv_heads - 1), work[0], slot_of(k, i + 1))
            elif k + 1 < kv_heads:
                scores(k + 1, work[0], slot_of(k, i + 1))
            absorb(k, r, slot_of(k, i))

    if unrolled or len(work) % 2:
        for k in range(kv_heads):
            one_head(k)
    else:
        pl.loop(0, kv_heads)(one_head)


def attention(queries, blocks, lift, state, group, pieces, window=None):
    heads, rows, _ = queries.shape
    kv_heads = heads // group
    low, high = window or (0, rows)
    chunk = min(high - low, 256)
    final = pieces > 0
    spans = [b[1:] for b in blocks]
    keys = sum(end - first for first, _, end in spans)
    lifted = any(end > middle for _, middle, end in spans)
    args = [queries] + [b[0] for b in blocks]
    in_specs = [IN_VMEM] * len(args)
    if lifted:
        in_specs.append(IN_VMEM)
        args.append(lift)
    if state is not None:
        in_specs.append(IN_VMEM)
        args.append(state)
    if final:
        out_shape = [jax.ShapeDtypeStruct(((high - low) // pieces, heads * HEAD), BF16)] * pieces
    else:
        out_shape = [jax.ShapeDtypeStruct((heads, STATE, rows), F32)]
    out = pl.pallas_call(
        functools.partial(
            attention_kernel, spans, lifted, state is not None, final, group, chunk, (low, high), True
        ),
        in_specs=in_specs,
        out_specs=[IN_VMEM] * len(out_shape),
        out_shape=out_shape,
        scratch_shapes=[
            pltpu.VMEM((kv_heads, STATE, keys), BF16),
            pltpu.VMEM((keys, group * chunk), F32),
            pltpu.VMEM((keys, group * chunk), F32),
        ],
        compiler_params=pltpu.CompilerParams(vmem_limit_bytes=VMEM_LIMIT),
        cost_estimate=cost(16 * heads * rows * keys * HEAD, 4 * heads * rows * TILE),
        name="attention",
    )(*args)
    return list(out) if final else out[0]


def output_kernel(count, *refs):
    attended = refs[:count]
    weights = refs[count : 2 * count]
    rest = refs[2 * count : -3] if len(refs) > 2 * count + 1 else ()
    out = refs[-3] if rest else refs[-1]
    step = min(out.shape[1], 4 * TILE)
    copies = []
    for i in range(0, out.shape[1], step):
        total = None
        for a, w in zip(attended, weights):
            term = dot(a[...], w[:, i : i + step])
            total = term if total is None else total + term
        if rest:
            begun, latent, mod = rest
            gate = [mod[t, 2:3, :] for t in range(mod.shape[0])]
            gate = jnp.concatenate(gate, axis=1)[:, i : i + step]
            total = latent[:, i : i + step].astype(F32) + gate * (begun[:, i : i + step] + total)
            made, sems = refs[-2:]
            made[:, i : i + step] = total.astype(out.dtype)
            lanes = pl.ds(i, step)
            copy = pltpu.make_async_copy(made.at[:, lanes], out.at[:, lanes], sems.at[i // step])
            copy.start()
            copies.append(copy)
        else:
            out[:, i : i + step] = total
    for copy in copies:
        copy.wait()


def project(attended, weights, begun, latent, mod, depth):
    count = len(attended)
    rows, inner = attended[0].shape
    rest = [] if begun is None else [begun, latent, mod]
    return pl.pallas_call(
        functools.partial(output_kernel, count),
        in_specs=[IN_VMEM] * (2 * count + len(rest)),
        out_specs=pl.BlockSpec(memory_space=pltpu.HBM) if rest else IN_VMEM,
        out_shape=jax.ShapeDtypeStruct((rows, depth), BF16 if rest else F32),
        scratch_shapes=[
            pltpu.VMEM((rows, depth), BF16),
            pltpu.SemaphoreType.DMA((pl.cdiv(depth, 4 * TILE),)),
        ]
        if rest
        else [],
        compiler_params=pltpu.CompilerParams(vmem_limit_bytes=VMEM_LIMIT),
        cost_estimate=cost(2 * rows * depth * inner * count, 2 * depth * inner * count),
        name="output",
    )(*attended, *weights, *rest)


def rotary_tables(rank, tp, rows, context_rows):
    index = lax.broadcasted_iota(jnp.int32, (tp * rows + context_rows, TILE), 0)
    lane = lax.broadcasted_iota(jnp.int32, (tp * rows + context_rows, TILE), 1)
    piece = index // rows
    position = (rank // tp * tp + jnp.bitwise_xor(rank % tp, piece)) * rows + index % rows
    quarter = HEAD // 4
    pair = lane % HEAD // 2
    frequency = ROTARY_BASE ** (-(pair % quarter).astype(F32) / quarter)
    place = jnp.where(pair < quarter, position // GRID, position % GRID).astype(F32)
    angle = jnp.where(index < tp * rows, place, 0.0) * frequency
    sine = jnp.sin(angle)
    even = lane % 2 == 0
    return jnp.cos(angle), jnp.where(even, -sine, 0.0), jnp.where(even, 0.0, sine)


def far_calls(tp, rows):
    each = min(tp // 2, max(1, TILE // rows))
    return each, tp // 2 // each


def shards(
    sp,
    tp,
    latent,
    context,
    conditioning,
    context_conditioning,
    shift_weight,
    scale_weight,
    gate_weight,
    norm_gain,
    query_weight,
    key_weight,
    value_weight,
    query_gain,
    key_gain,
    context_lift,
    output_weight,
):
    rows = latent.shape[0]
    length = rows * tp
    context_rows = context.shape[0]
    group = query_weight.shape[1] // key_weight.shape[1]
    tp_bits = [1 << b for b in reversed(range(tp.bit_length() - 1))]

    def spread(have, bit):
        have.update({j | bit: swap(v, "tp", tp, bit) for j, v in list(have.items())})

    def tie(*values):
        return lax.optimization_barrier(values)

    pieces = {0: latent}
    spread(pieces, tp_bits[0])
    partial = modulation_partial(
        conditioning, context_conditioning, shift_weight, scale_weight, gate_weight
    )
    rank = lax.axis_index("sp") * tp + lax.axis_index("tp")
    gains = [v.reshape(1, -1) for v in (norm_gain, key_gain, query_gain)]
    early = [
        (*rotary_tables(rank, tp, rows, context_rows), jnp.concatenate(gains, axis=1)),
        (
            jnp.concatenate([key_weight, value_weight], axis=1),
            jnp.broadcast_to(context_lift[:, None, None], context_lift.shape + (8, TILE)),
        ),
    ]
    ready = []
    bits = [1 << b for b in range(sp.bit_length() - 1)]
    for i in range(0, len(bits), 2):
        pair = bits[i : i + 2]
        masks = pair + [sum(pair)] if len(pair) == 2 else pair
        arrived = []
        for m in masks:
            arrived.append(swap(partial, "sp", sp, m))
        extra = early.pop(0) if early else ()
        tied = tie(*arrived, *extra)
        partial = sum(tied[: len(arrived)], partial)
        ready += tied[len(arrived) :]
    for extra in early:
        ready += extra
    *tables, gains, kv_weight, lifts = ready
    partial, pieces[tp_bits[0]] = tie(partial, pieces[tp_bits[0]])
    for bit in tp_bits[1:]:
        spread(pieces, bit)
    tails = {0: partial}
    for j in reversed(range(1, tp)):
        tails[j] = swap(partial, "tp", tp, j)

    normal = normal_rows([pieces[j] for j in range(tp)] + [context])
    tails = [tails[j] for j in range(tp)]
    hidden, first, second, mod = keys_values(
        normal, context_rows, tails, gains, kv_weight, tables
    )

    half = length // 2
    order = list(range(0, sp, 2)) + list(range(sp - 1, 0, -2))
    ahead = [(order[i], order[(i + 1) % sp]) for i in range(sp)]
    back = [(b, a) for a, b in ahead]

    def hop(pair):
        return lax.ppermute(pair[0], "sp", ahead), lax.ppermute(pair[1], "sp", back)

    def as_blocks(pair):
        return [(b, 0, half, b.shape[0]) for b in pair]

    flight = [hop((first, second))]
    flight.append(hop((second, first)))
    queries = queries_of(hidden, query_weight, gains, tables, length)
    output_weight, _ = tie(output_weight, first)
    weights = {0: output_weight}
    spread(weights, tp_bits[0])
    waiting = as_blocks((first, second))
    state = None
    for i in range(sp - 1):
        state = attention(queries, waiting, lifts, state, group, 0)
        up, down, state = tie(*flight.pop(0), state)
        if i < sp - 3:
            flight.append(hop((up, down)))
        waiting = as_blocks((up, down))
    far = []
    each, calls = far_calls(tp, rows)
    for c in reversed(range(calls)):
        window = (half + c * each * rows, half + (c + 1) * each * rows)
        made = attention(queries, waiting, lifts, state, group, each, window)
        *made, state = tie(*made, state)
        made = [swap(a, "tp", tp, tp // 2 + c * each + j) for j, a in enumerate(made)]
        far = made + far
    top_bit = tp_bits[0]
    weights[top_bit], state = tie(weights[top_bit], state)
    for bit in tp_bits[1:]:
        spread(weights, bit)
    near = attention(queries, waiting, lifts, state, group, tp // 2, (0, half))
    near = near[:1] + [swap(a, "tp", tp, j) for j, a in enumerate(near) if j]
    weights = [weights[j] for j in range(tp)]
    begun = project(near, weights[: tp // 2], None, None, None, latent.shape[1])
    return project(far, weights[tp // 2 :], begun, latent, mod, latent.shape[1])


def solution(mesh):
    in_specs = (
        P(("sp", "tp"), None),
        P("sp", None),
        P("sp"),
        P("sp"),
        P("sp", "tp"),
        P("sp", "tp"),
        P("sp", "tp"),
        P(),
        P(None, "tp"),
        P(None, "tp"),
        P(None, "tp"),
        P(),
        P(),
        P("tp"),
        P("tp", None),
    )
    return jax.shard_map(
        functools.partial(shards, mesh.shape["sp"], mesh.shape["tp"]),
        mesh=mesh,
        in_specs=in_specs,
        out_specs=P(("sp", "tp"), None),
        check_vma=False,
    )
```
